32 devices in a mesh: grp: 2 (over y), sp: 4 (over z), tp: 4 (over x, core).
Axes of the slice: x: 2, y: 2, z: 4, core: 2. Of those that a mesh axis runs over, the one named last changes fastest.
Arguments:
- tokens: bfloat16 [2048, 2048], P(('grp', 'sp', 'tp')), parts along dimension 0, may hold values from -6 to 6
- norm_gain: float32 [2048], replicated, may hold values from 0.1 to 1.9
- conv_b_w: bfloat16 [2048, 1024], P('sp', 'tp'), may hold values from -0.125 to 0.125
- conv_c_w: bfloat16 [2048, 1024], P('sp', 'tp'), may hold values from -0.125 to 0.125
- conv_x_w: bfloat16 [2048, 1024], P('sp', 'tp'), may hold values from -0.125 to 0.125
- query_w: bfloat16 [2048, 1024], P('sp', 'tp'), may hold values from -1 to 1
- key_w: bfloat16 [2048, 256], P('sp', 'tp'), may hold values from -2 to 2
- value_w: bfloat16 [2048, 256], P('sp', 'tp'), may hold values from -0.125 to 0.125
- conv_taps: float32 [3, 1024], P(None, 'tp'), may hold values from -3.5 to 3.5
- gate_cache: float32 [2048, 16], P('grp', 'tp'), parts along dimension 0, as said below
- out_conv_w: bfloat16 [1024, 2048], P('tp'), may hold values from -0.1875 to 0.1875
- out_attn_w: bfloat16 [1024, 2048], P('tp'), may hold values from -0.75 to 0.75
Outputs:
- mixed: bfloat16 [2048, 2048], P(('grp', 'sp', 'tp')), parts along dimension 0
- log_total: float32 [2048, 16], P(('grp', 'sp'), 'tp'), parts along dimension 0
The draws below stay inside these ranges and needn't reach their ends.
There are 2 independent parts, one for each index of `grp`. The reference program is written for one: setup_inputs(seed, part) draws one part's arguments, and reference() takes and returns one part's arrays. A program takes and returns all parts, laid end to end along the dimension named above; an argument that names none is the same for every part. Nothing has to cross between parts.
Inputs may be any that keep to these rules, and one draw needn't show every extreme that they name: `gate_cache`: never rises along positions; starts at or below zero.
All inputs are finite; a program needn't handle non-finite values.
Results may differ from the reference program's by a relative error of at most 0.017.
The reference program's roundings to bfloat16 on the way count: a program that leaves them out, or rounds other values in their place, can miss the bound.
Values may be sent and summed in bfloat16 or wider, within the bound.
No kernel may reach another device: no remote copies, remote signals or barrier semaphores. Data moves between devices by JAX's collectives and lax.ppermute only.
A program may use at most 64 MiB of HBM per device.

```python
import jax
import jax.numpy as jnp
from jax import lax

D = 2048
CONV = 1024
QH = 16
KVH = 4
HD = 64
CW = 3
TOK_DEV = 256
SEQUENCE_LENGTH = 1024
N_TP = 4


def query_key_pair(key):
    base = jax.random.fold_in(key, 11)
    first, second = jax.random.split(base)
    query_f = jnp.clip(jax.random.normal(first, (D, QH * HD), jnp.float32), -5.0, 5.0) * D ** (-0.5)
    noise = jnp.clip(jax.random.normal(second, (D, KVH * HD), jnp.float32), -5.0, 5.0) * D ** (-0.5)
    key_f = noise
    return (query_f, jnp.clip(key_f, -2.0, 2.0))


def draw_query_w(key, part):
    pair = query_key_pair(key)
    return pair[0].astype(jnp.bfloat16)


def draw_key_w(key, part):
    pair = query_key_pair(key)
    return pair[1].astype(jnp.bfloat16)


def draw_gate_cache(key, part):
    keys = jax.random.split(key, 7)
    order = jax.random.permutation(keys[0], QH)
    fast = order < QH // 2
    fast_rate = 1.0 / 40.0 * jnp.exp(jax.random.uniform(keys[1], (QH,), jnp.float32, -0.5, 0.5))
    slow_rate = 0.6 / SEQUENCE_LENGTH * jnp.exp(jax.random.uniform(keys[6], (QH,), jnp.float32, -0.5, 0.5))
    decay_speed = jnp.where(fast, fast_rate, slow_rate)
    blocks = SEQUENCE_LENGTH // TOK_DEV
    scale_per_block = jnp.exp(jax.random.uniform(keys[2], (blocks, QH), jnp.float32, -0.9, 0.9))
    scale_per_block = jnp.repeat(scale_per_block, TOK_DEV, axis=0)
    coarse_estimate = jnp.exp(jax.random.uniform(keys[3], (SEQUENCE_LENGTH, QH), jnp.float32, -1.0, 1.0))
    chosen_locations = jax.random.randint(keys[4], (3,), 0, SEQUENCE_LENGTH)
    spike_amplitude = jnp.zeros((SEQUENCE_LENGTH,), jnp.float32).at[chosen_locations].set(1.0)
    objective_value = jax.random.uniform(keys[5], (QH,), jnp.float32, 0.2, 0.5) * (1.0 - fast.astype(jnp.float32))
    gate_logarithm = -(decay_speed[None, :] * scale_per_block * coarse_estimate + spike_amplitude[:, None] * objective_value[None, :])
    return jnp.cumsum(gate_logarithm, axis=0)


def levels(stream_key, extent, cuts, low, largest):
    loudness, own = 1.0, jax.random.fold_in(stream_key, 6)
    for dim, parts in cuts:
        steps = jnp.exp(jax.random.uniform(jax.random.fold_in(own, dim), (parts,), jnp.float32, low / len(cuts), largest / len(cuts)))
        loudness = loudness * jnp.repeat(steps, extent[dim] // parts).reshape([-1 if axis == dim else 1 for axis in range(len(extent))])
    return loudness


def bell_draw(key, dims, deviation, most, cuts=(), held_as=jnp.bfloat16):
    gain = levels(key, dims, cuts, -0.22, 0.18) if cuts else 1.0
    values = jax.random.normal(key, dims, jnp.float32) * deviation * gain
    return jnp.minimum(jnp.maximum(values, -most), most).astype(held_as)


def setup_inputs(seed: int = 0, part: int = 0) -> dict:
    seeds = jax.random.split(jax.random.key(seed), 13)
    part_splits = jax.random.split(jax.random.fold_in(seeds[12], part), 13)
    return {
        "tokens": bell_draw(part_splits[0], (SEQUENCE_LENGTH, D), 1.0, 6.0, ((0, 16),)),
        "norm_gain": jnp.clip(1.0 + 0.18 * jax.random.normal(seeds[1], (D,), jnp.float32), 0.1, 1.9),
        "conv_b_w": bell_draw(seeds[2], (D, CONV), D ** -0.5, 0.125, ((0, 4), (1, 4))),
        "conv_c_w": bell_draw(seeds[3], (D, CONV), D ** -0.5, 0.125, ((0, 4), (1, 4))),
        "conv_x_w": bell_draw(seeds[4], (D, CONV), D ** -0.5, 0.125, ((0, 4), (1, 4))),
        "query_w": draw_query_w(jax.random.fold_in(seeds[12], 71), part),
        "key_w": draw_key_w(jax.random.fold_in(seeds[12], 71), part),
        "value_w": bell_draw(seeds[7], (D, KVH * HD), D ** -0.5, 0.125, ((0, 4), (1, 4))),
        "conv_taps": bell_draw(seeds[8], (CW, CONV), CW ** -0.5, 3.5, ((1, 4),), jnp.float32),
        "gate_cache": draw_gate_cache(jax.random.fold_in(jax.random.fold_in(seeds[12], part), 71), part),
        "out_conv_w": bell_draw(seeds[10], (CONV, D), CONV ** -0.5, 0.1875, ((0, 4),)),
        "out_attn_w": bell_draw(seeds[11], (QH * HD, D), (QH * HD // 16) ** -0.5, 0.75, ((0, 4),)),
    }


def reference(tokens, norm_gain, conv_b_w, conv_c_w, conv_x_w, query_w, key_w, value_w, conv_taps, gate_cache, out_conv_w, out_attn_w):
    xf = tokens.astype(jnp.float32)
    scale_rows = lax.rsqrt(lax.optimization_barrier(jnp.mean(xf * xf, axis=-1, keepdims=True)) + 1e-05)
    normed = (xf * norm_gain).astype(jnp.bfloat16)

    def project(weight):
        return (jnp.dot(normed, weight, preferred_element_type=jnp.float32) * scale_rows).astype(jnp.bfloat16)
    gate_b = project(conv_b_w)
    gate_c = project(conv_c_w)
    conv_in = project(conv_x_w)
    query = project(query_w)
    key = project(key_w)
    value = project(value_w)
    conv_src = (gate_c.astype(jnp.float32) * conv_in.astype(jnp.float32)).astype(jnp.bfloat16)
    padded = jnp.concatenate([jnp.zeros((CW - 1, CONV), jnp.bfloat16), conv_src], axis=0)
    filtered = jnp.zeros((SEQUENCE_LENGTH, CONV), jnp.float32)
    for tap in range(CW):
        filtered = filtered + conv_taps[tap][None, :] * padded[tap:tap + SEQUENCE_LENGTH].astype(jnp.float32)
    conv_out = (gate_b.astype(jnp.float32) * filtered).astype(jnp.bfloat16)
    group = QH // KVH
    q_block = min(256, SEQUENCE_LENGTH)
    n_blocks = SEQUENCE_LENGTH // q_block
    heads_q = query.reshape(SEQUENCE_LENGTH, KVH, group, HD)
    keys_f = key.reshape(SEQUENCE_LENGTH, KVH, HD).astype(jnp.float32)
    values_f = value.reshape(SEQUENCE_LENGTH, KVH, HD).astype(jnp.float32)
    key_gate = gate_cache.T.reshape(KVH, group, 1, SEQUENCE_LENGTH)
    key_pos = jnp.arange(SEQUENCE_LENGTH, dtype=jnp.int32)

    def attend(index):
        begin = (index * q_block).astype(jnp.int32)
        q_rows = lax.dynamic_slice_in_dim(heads_q, begin, q_block, 0).astype(jnp.float32)
        q_gate = lax.dynamic_slice_in_dim(gate_cache, begin, q_block, 0)
        score = jnp.einsum('qgjd,kgd->gjqk', q_rows, keys_f) * HD ** (-0.5)
        score = score + q_gate.T.reshape(KVH, group, q_block, 1) - key_gate
        q_pos = begin + jnp.arange(q_block, dtype=jnp.int32)
        mask = key_pos[None, :] <= q_pos[:, None]
        score = jnp.where(mask, score, -1e+30)
        row_max = lax.optimization_barrier(jnp.max(score, axis=-1))
        weight = jnp.where(mask, jnp.exp(score - row_max[..., None]), 0.0)
        row_sum = lax.optimization_barrier(jnp.sum(weight, axis=-1))
        weight_bf = lax.optimization_barrier(weight.astype(jnp.bfloat16)).astype(jnp.float32)
        summed = jnp.einsum('gjqk,kgd->gjqd', weight_bf, values_f) / row_sum[..., None]
        out = summed.transpose(2, 0, 1, 3).reshape(q_block, QH * HD).astype(jnp.bfloat16)
        lse = (row_max + jnp.log(row_sum)).transpose(2, 0, 1).reshape(q_block, QH)
        return (out, lse)
    outs, lses = lax.map(attend, jnp.arange(n_blocks, dtype=jnp.int32))
    attn_out = outs.reshape(SEQUENCE_LENGTH, QH * HD)
    log_total = lses.reshape(SEQUENCE_LENGTH, QH)
    conv_part = CONV // N_TP
    attn_part = QH * HD // N_TP
    mixed = jnp.zeros((SEQUENCE_LENGTH, D), jnp.float32)
    for part in range(N_TP):
        term = jnp.dot(conv_out[:, part * conv_part:(part + 1) * conv_part], out_conv_w[part * conv_part:(part + 1) * conv_part], preferred_element_type=jnp.float32)
        term = term + jnp.dot(attn_out[:, part * attn_part:(part + 1) * attn_part], out_attn_w[part * attn_part:(part + 1) * attn_part], preferred_element_type=jnp.float32)
        mixed = mixed + term.astype(jnp.bfloat16).astype(jnp.float32)
    return (mixed.astype(jnp.bfloat16), log_total)
```

```python
import functools

import jax
import jax.numpy as jnp
from jax import lax
from jax.experimental import pallas as pl
from jax.experimental.pallas import tpu as pltpu
from jax.sharding import PartitionSpec as P

HD = 64
LANES = 128
EPS = 1e-05
VMEM = pl.BlockSpec(memory_space=pltpu.VMEM)
SMEM = pl.BlockSpec(memory_space=pltpu.SMEM)


def passed_along(value, axis, by):
    count = lax.axis_size(axis)
    pairs = [(i, i + by) for i in range(count) if 0 <= i + by < count]
    return lax.ppermute(value, axis, pairs)


def by_rows(
    tokens,
    norm_gain,
    conv_b_w,
    conv_c_w,
    conv_x_w,
    query_w,
    key_w,
    value_w,
    conv_taps,
    gate_cache,
    out_conv_w,
    out_attn_w,
):
    rows = lax.all_gather(tokens, "tp", axis=0, tiled=True)
    count = rows.shape[0]
    xf = rows.astype(jnp.float32)
    scale_rows = lax.rsqrt(jnp.mean(xf * xf, axis=-1, keepdims=True) + 1e-05)
    normed = (xf * norm_gain).astype(jnp.bfloat16)

    def contract_all(pieces):
        width = pieces[0].shape[0]
        return tuple(
            (jnp.dot(normed, piece, preferred_element_type=jnp.float32) for piece in pieces)
        )

    conv_sums = contract_all(
        (
            lax.all_gather(conv_b_w, "sp", axis=0, tiled=True),
            lax.all_gather(conv_c_w, "sp", axis=0, tiled=True),
            lax.all_gather(conv_x_w, "sp", axis=0, tiled=True),
        )
    )
    attn_sums = contract_all(
        (
            lax.all_gather(query_w, "sp", axis=0, tiled=True),
            lax.all_gather(key_w, "sp", axis=0, tiled=True),
            lax.all_gather(value_w, "sp", axis=0, tiled=True),
        )
    )
    sums = conv_sums + attn_sums
    gate_b, gate_c, conv_in, query, key, value = [
        (total * scale_rows).astype(jnp.bfloat16) for total in sums
    ]
    taps = conv_taps.shape[0]
    channels = conv_in.shape[1]
    conv_src = (gate_c.astype(jnp.float32) * conv_in.astype(jnp.float32)).astype(jnp.bfloat16)
    earlier = passed_along(conv_src[count - (taps - 1) :], "sp", 1)
    padded = jnp.concatenate([earlier, conv_src], axis=0)
    filtered = jnp.zeros((count, channels), jnp.float32)
    for tap in range(taps):
        filtered = filtered + conv_taps[tap][None, :] * padded[tap : tap + count].astype(
            jnp.float32
        )
    conv_out = (gate_b.astype(jnp.float32) * filtered).astype(jnp.bfloat16)
    heads_dev = gate_cache.shape[1]
    kv_dev = key.shape[1] // HD
    group = heads_dev // kv_dev
    half = count // 2
    sp_index = lax.axis_index("sp")
    own_start = sp_index * count
    scale = HD ** (-0.5)
    later_query = query[half:]
    later_start = own_start + half

    def prepare(q_rows, begin):
        heads_q = q_rows.reshape(half, kv_dev, group, HD)
        q_gate = lax.dynamic_slice_in_dim(gate_cache, begin, half, 0).T.reshape(
            kv_dev, group, half, 1
        )
        q_pos = begin + jnp.arange(half, dtype=jnp.int32)
        return (heads_q, q_gate, q_pos)

    sides = (prepare(query[:half], own_start), prepare(later_query, later_start))

    def absorb(carry, side, key_rows, value_rows, begin):
        heads_q, q_gate, q_pos = side
        run_max, run_sum, acc = carry
        width = key_rows.shape[0]
        key_heads = key_rows.reshape(width, kv_dev, HD)
        value_heads = value_rows.reshape(width, kv_dev, HD)
        score = (
            jnp.einsum("qgjd,kgd->gjqk", heads_q, key_heads, preferred_element_type=jnp.float32)
            * scale
        )
        key_gate = lax.dynamic_slice_in_dim(gate_cache, begin, width, 0).T.reshape(
            kv_dev, group, 1, width
        )
        score = score + q_gate - key_gate
        mask = (begin + jnp.arange(width, dtype=jnp.int32))[None, :] <= q_pos[:, None]
        score = jnp.where(mask, score, -1e30)
        new_max = jnp.maximum(run_max, jnp.max(score, axis=-1))
        weight = jnp.where(mask, jnp.exp(score - new_max[..., None]), 0.0)
        factor = jnp.exp(run_max - new_max)
        new_sum = run_sum * factor + jnp.sum(weight, axis=-1)
        product = jnp.einsum(
            "gjqk,kgd->gjqd",
            weight.astype(jnp.bfloat16),
            value_heads,
            preferred_element_type=jnp.float32,
        )
        return (new_max, new_sum, acc * factor[..., None] + product)

    def guarded(carry, side, key_rows, value_rows, begin):

        def visit_rows(state):
            return absorb(state, side, key_rows, value_rows, begin)

        def keep(state):
            return state

        return lax.cond(begin <= side[2][half - 1], visit_rows, keep, carry)

    def absorb_both(carry, key_rows, value_rows, begin):
        return (
            guarded(carry[0], sides[0], key_rows, value_rows, begin),
            guarded(carry[1], sides[1], key_rows, value_rows, begin),
        )

    def fresh():
        return (
            jnp.full((kv_dev, group, half), -1e30, jnp.float32),
            jnp.zeros((kv_dev, group, half), jnp.float32),
            jnp.zeros((kv_dev, group, half, HD), jnp.float32),
        )

    key_rows = lax.all_gather(key, "sp", axis=0, tiled=True)
    value_rows = lax.all_gather(value, "sp", axis=0, tiled=True)
    width = key_rows.shape[0]
    step = 512
    key_blocks = key_rows.reshape(width // step, step, key_rows.shape[1])
    value_blocks = value_rows.reshape(width // step, step, value_rows.shape[1])
    firsts = step * jnp.arange(width // step, dtype=jnp.int32)

    def visit(state, inputs):
        return (absorb_both(state, inputs[0], inputs[1], inputs[2]), None)

    result, unused = lax.scan(visit, (fresh(), fresh()), (key_blocks, value_blocks, firsts))

    def finish(state):
        run_max, run_sum, acc = state
        out = (
            (acc / run_sum[..., None])
            .transpose(2, 0, 1, 3)
            .reshape(half, heads_dev * HD)
            .astype(jnp.bfloat16)
        )
        lse = (run_max + jnp.log(run_sum)).transpose(2, 0, 1).reshape(half, heads_dev)
        return (out, lse)

    early_out, early_lse = finish(result[0])
    later_out, later_lse = finish(result[1])
    attn_out = jnp.concatenate([early_out, later_out], axis=0)
    log_total = jnp.concatenate([early_lse, later_lse], axis=0)
    term = jnp.dot(conv_out, out_conv_w, preferred_element_type=jnp.float32)
    mixed = lax.psum_scatter(
        (term + jnp.dot(attn_out, out_attn_w, preferred_element_type=jnp.float32)).astype(
            jnp.bfloat16
        ),
        "tp",
        scatter_dimension=0,
        tiled=True,
    )
    return (mixed, log_total)


def shape(dims, dtype=jnp.bfloat16):
    return jax.ShapeDtypeStruct(dims, dtype)


def run(kernel, where, operands, outs, scratch, name, flops, nbytes):
    return pl.pallas_call(
        kernel,
        out_shape=outs,
        in_specs=[SMEM] + [VMEM] * len(operands),
        out_specs=jax.tree.map(lambda unused: VMEM, outs),
        scratch_shapes=scratch,
        name=name,
        cost_estimate=pl.CostEstimate(flops=flops, bytes_accessed=nbytes, transcendentals=0),
    )(where, *operands)


def low_half(width):
    return lax.broadcasted_iota(jnp.int32, (1, width), 1) < width // 2


def pack_kernel(n, at, b_ref, c_ref, x_ref, q_ref, k_ref, v_ref, *outs):
    own, part = at[0], at[2]

    def both(ref):
        turned = ref[...].astype(jnp.float32)
        return jnp.concatenate([turned, turned], axis=0).T

    key, value = both(k_ref), both(v_ref)
    low = low_half(LANES)
    for step in range(n):
        to = lax.rem(own + step, n)
        tile = pl.ds(pl.multiple_of((to // 2) * LANES, LANES), LANES)
        odd = (to % 2) == 1

        def sides(ref):
            plain = ref[:, tile].astype(jnp.float32)
            return plain, pltpu.roll(plain, LANES // 2, 1)

        def lower(ref):
            plain, rolled = sides(ref)
            return jnp.where(odd, rolled, plain)

        def upper(ref):
            plain, rolled = sides(ref)
            return jnp.where(odd, plain, rolled)

        tiles = (
            jnp.where(low, lower(b_ref), upper(q_ref)),
            jnp.where(low, lower(c_ref), key),
            jnp.where(low, lower(x_ref), value),
        )
        for index, full in enumerate(tiles):
            columns = slice(index * LANES, (index + 1) * LANES)
            full = full.astype(jnp.bfloat16)
            out = outs[step]
            if step == 0:
                out[:, columns] = full
            else:
                half = out.shape[0]
                out[:, columns] = jnp.where(part == 0, full[:half], full[half:])


def project_kernel(n, at, gain_ref, t0, t1, t2, t3, *rest):
    weights, (out, normed, scales) = rest[: 2 * n - 1], rest[2 * n - 1 :]
    own, column, part = at[0], at[1], at[2]
    gain = gain_ref[...]
    for index, ref in enumerate((t0, t1, t2, t3)):
        count = ref.shape[0]
        rows = pl.ds(pl.multiple_of((column ^ index) * count, count), count)
        xf = ref[...].astype(jnp.float32)
        scale = lax.rsqrt(jnp.mean(xf * xf, axis=-1, keepdims=True) + EPS)
        scales[rows, :] = jnp.broadcast_to(scale, (count, LANES))
        normed[rows, :] = (xf * gain).astype(jnp.bfloat16)

    def term(start, ref):
        depth = ref.shape[0]
        columns = pl.ds(pl.multiple_of(start, depth), depth)
        return jnp.dot(normed[:, columns], ref[...], preferred_element_type=jnp.float32)

    depth = weights[0].shape[0]
    total = term(own * depth, weights[0])
    for step in range(1, n):
        start = lax.rem(own + n - step, n) * depth
        half = depth // 2
        total = total + term(start + part * half, weights[2 * step - 1])
        total = total + term(start + (1 - part) * half, weights[2 * step])
    scale = scales[...][:, :1]
    out[...] = (total * scale).astype(jnp.bfloat16)


def mix_kernel(n, at, p0, p1, p2, p3, taps_ref, gate_ref, *rest):
    outs, sums = rest[:n], rest[n : 2 * n]
    held, source, mixed, lse = rest[2 * n :]
    own = at[0]
    count = p0.shape[0]
    rows_all = n * count
    for step, ref in enumerate((p0, p1, p2, p3)):
        begin = lax.rem(own + n - step, n) * count
        held[pl.ds(pl.multiple_of(begin, count), count), :] = ref[...]
    low = low_half(LANES)
    lead = source.shape[0] - rows_all
    source[:lead, :] = jnp.zeros((lead, LANES), jnp.float32)
    gated = held[:, LANES : 2 * LANES].astype(jnp.float32) * held[:, 2 * LANES :].astype(jnp.float32)
    source[lead:, :] = gated.astype(jnp.bfloat16).astype(jnp.float32)
    taps_n = taps_ref.shape[0]
    tile = pl.ds(pl.multiple_of((own // 2) * LANES, LANES), LANES)
    taps = taps_ref[:, tile]
    taps = jnp.where((own % 2) == 1, pltpu.roll(taps, LANES // 2, 1), taps)
    gate_row = gate_ref[pl.ds(own, 1), :]
    gate_column = jnp.broadcast_to(gate_row, (LANES, rows_all)).T
    scale = HD ** (-0.5)
    ahead = lax.broadcasted_iota(jnp.int32, (count, count), 0) >= lax.broadcasted_iota(
        jnp.int32, (count, count), 1
    )
    for block in range(n):
        first = block * count
        last = first + count
        filtered = jnp.zeros((count, LANES), jnp.float32)
        for tap in range(taps_n):
            begin = lead + first + tap - (taps_n - 1)
            filtered = filtered + taps[tap : tap + 1, :] * source[begin : begin + count, :]
        front = held[first:last, :LANES]
        conv = front.astype(jnp.float32) * filtered
        query = jnp.where(low, jnp.zeros_like(front), front)
        score = (
            lax.dot_general(
                query,
                held[:last, LANES : 2 * LANES],
                (((1,), (1,)), ((), ())),
                preferred_element_type=jnp.float32,
            )
            * scale
        )
        score = score + gate_column[first:last, :1] - gate_row[:, :last]
        edge = jnp.where(ahead, score[:, first:], -1e30)
        if block:
            before = score[:, :first]
            top = jnp.maximum(
                jnp.max(before, axis=-1, keepdims=True), jnp.max(edge, axis=-1, keepdims=True)
            )
            weight = jnp.concatenate([jnp.exp(before - top), jnp.exp(edge - top)], axis=1)
        else:
            top = jnp.max(edge, axis=-1, keepdims=True)
            weight = jnp.exp(edge - top)
        total = jnp.sum(weight, axis=-1, keepdims=True)
        product = jnp.dot(
            weight.astype(jnp.bfloat16),
            held[:last, 2 * LANES :],
            preferred_element_type=jnp.float32,
        )
        mixed[first:last, :] = jnp.where(low, conv, product / total).astype(jnp.bfloat16)
        lse[block : block + 1, :] = jnp.broadcast_to(top + jnp.log(total), (count, LANES)).T[:1, :]
    for step in range(n):
        to = lax.rem(own + step, n)
        outs[step][...] = mixed[pl.ds(pl.multiple_of(to * count, count), count), :]
        sums[step][...] = lse[pl.ds(to, 1), :]


def out_kernel(n, at, a0, a1, a2, a3, conv_w, attn_w, *rest):
    outs, (joined, weights, partial) = rest[:-3], rest[-3:]
    own, column = at[0], at[1]
    for step, ref in enumerate((a0, a1, a2, a3)):
        part = lax.rem(own + n - step, n)
        begin = pl.multiple_of(part * HD, HD)
        joined[:, step * LANES : (step + 1) * LANES] = ref[...]
        weights[step * LANES : step * LANES + HD, :] = conv_w[pl.ds(begin, HD), :]
        weights[step * LANES + HD : (step + 1) * LANES, :] = attn_w[pl.ds(begin, HD), :]
    partial[...] = jnp.dot(
        joined[...], weights[...], preferred_element_type=jnp.float32
    ).astype(jnp.bfloat16)
    for index, out in enumerate(outs):
        count = out.shape[0]
        out[...] = partial[pl.ds(pl.multiple_of((column ^ index) * count, count), count), :]


def by_columns(
    tokens,
    norm_gain,
    conv_b_w,
    conv_c_w,
    conv_x_w,
    query_w,
    key_w,
    value_w,
    conv_taps,
    gate_cache,
    out_conv_w,
    out_attn_w,
):
    n, n_tp = lax.axis_size("sp"), lax.axis_size("tp")
    where = jnp.stack([lax.axis_index("sp"), lax.axis_index("tp"), lax.axis_index("grp")])
    where = where.astype(jnp.int32)
    round_sp = lambda step: [(i, (i + step) % n) for i in range(n)]
    swap_tp = lambda bit: [(i, i ^ bit) for i in range(n_tp)]
    m, d = tokens.shape
    depth, width = conv_b_w.shape
    packed = 3 * LANES
    half = depth // 2
    own_w, *sends = run(
        functools.partial(pack_kernel, n),
        where,
        (conv_b_w, conv_c_w, conv_x_w, query_w, key_w.T, value_w.T),
        [shape((depth, packed))] + [shape((half, packed))] * (n - 1),
        [],
        "pack",
        depth * packed * n,
        6 * depth * width,
    )
    weights = [own_w]
    for step, value in zip(range(1, n), sends):
        came = lax.ppermute(value, "sp", round_sp(step))
        weights += [came, lax.ppermute(came, "grp", [(0, 1), (1, 0)])]
    gain = norm_gain.reshape(1, d)
    blocks = []
    for step in range(n):
        mine = tokens if step == 0 else lax.ppermute(tokens, "sp", round_sp(step))
        over = lax.ppermute(mine, "tp", swap_tp(2))
        side = lax.ppermute(mine, "tp", swap_tp(1))
        cross = lax.ppermute(over, "tp", swap_tp(1))
        blocks.append(
            run(
                functools.partial(project_kernel, n),
                where,
                (gain, mine, side, over, cross, *weights),
                shape((m * n_tp, packed)),
                [pltpu.VMEM((m * n_tp, d), jnp.bfloat16), pltpu.VMEM((m * n_tp, LANES), jnp.float32)],
                f"project{step}",
                2 * m * n_tp * d * packed,
                2 * (m * n_tp + packed) * d,
            )
        )
    count = m * n_tp
    rows = n * count
    results = run(
        functools.partial(mix_kernel, n),
        where,
        (*blocks, conv_taps, gate_cache.T),
        [shape((count, LANES))] * n + [shape((1, count), jnp.float32)] * n,
        [
            pltpu.VMEM((rows, packed), jnp.bfloat16),
            pltpu.VMEM((rows + 8, LANES), jnp.float32),
            pltpu.VMEM((rows, LANES), jnp.bfloat16),
            pltpu.VMEM((n, count), jnp.float32),
        ],
        "mix",
        4 * rows * rows * LANES,
        2 * rows * packed,
    )
    parts, sums = results[:n], results[n:]
    parts = [parts[0]] + [lax.ppermute(parts[k], "sp", round_sp(k)) for k in range(1, n)]
    sums = [sums[0]] + [lax.ppermute(sums[k], "sp", round_sp(k)) for k in range(1, n)]
    partials = run(
        functools.partial(out_kernel, n),
        where,
        (*parts, out_conv_w, out_attn_w),
        [shape((m, d))] * n_tp,
        [
            pltpu.VMEM((count, n * LANES), jnp.bfloat16),
            pltpu.VMEM((n * LANES, d), jnp.bfloat16),
            pltpu.VMEM((count, d), jnp.bfloat16),
        ],
        "output",
        2 * count * n * LANES * d,
        4 * n * LANES * d,
    )
    total = partials[0].astype(jnp.float32)
    for index in (1, 2, 3):
        total = total + lax.ppermute(partials[index], "tp", swap_tp(index)).astype(jnp.float32)
    mixed = total.astype(jnp.bfloat16)
    stacked = jnp.concatenate(sums, axis=0)
    order = jnp.mod(lax.axis_index("sp") - jnp.arange(n), n)
    log_total = jnp.take(stacked, order, axis=0).T
    return (mixed, log_total)


def on_device(*operands):
    tokens, key_w, gate_cache = operands[0], operands[6], operands[9]
    n, n_tp, n_grp = (lax.axis_size(name) for name in ("sp", "tp", "grp"))
    channels = operands[2].shape[1]
    heads = gate_cache.shape[1]
    fits = (
        n == heads
        and n_tp == 4
        and n_grp == 2
        and key_w.shape[1] == HD
        and channels == n * HD
        and 2 * HD == LANES
        and gate_cache.shape[0] == n * n_tp * tokens.shape[0]
    )
    return (by_columns if fits else by_rows)(*operands)


def solution(mesh):
    placed = (
        P(("grp", "sp", "tp"), None),
        P(),
        P("sp", "tp"),
        P("sp", "tp"),
        P("sp", "tp"),
        P("sp", "tp"),
        P("sp", "tp"),
        P("sp", "tp"),
        P(None, "tp"),
        P("grp", "tp"),
        P("tp", None),
        P("tp", None),
    )
    return jax.shard_map(
        on_device,
        mesh=mesh,
        in_specs=placed,
        out_specs=(P(("grp", "sp", "tp"), None), P(("grp", "sp"), "tp")),
        check_vma=False,
    )
```

```python
import functools

import jax
import jax.numpy as jnp
from jax import lax
from jax.experimental import pallas as pl
from jax.experimental.pallas import tpu as pltpu
from jax.sharding import PartitionSpec as P

HD = 64
LANES = 128
EPS = 1e-05
VMEM = pl.BlockSpec(memory_space=pltpu.VMEM)
SMEM = pl.BlockSpec(memory_space=pltpu.SMEM)


def passed_along(value, axis, by):
    count = lax.axis_size(axis)
    pairs = [(i, i + by) for i in range(count) if 0 <= i + by < count]
    return lax.ppermute(value, axis, pairs)


def by_rows(
    tokens,
    norm_gain,
    conv_b_w,
    conv_c_w,
    conv_x_w,
    query_w,
    key_w,
    value_w,
    conv_taps,
    gate_cache,
    out_conv_w,
    out_attn_w,
):
    rows = lax.all_gather(tokens, "tp", axis=0, tiled=True)
    count = rows.shape[0]
    xf = rows.astype(jnp.float32)
    scale_rows = lax.rsqrt(jnp.mean(xf * xf, axis=-1, keepdims=True) + 1e-05)
    normed = (xf * norm_gain).astype(jnp.bfloat16)

    def contract_all(pieces):
        return tuple(
            (jnp.dot(normed, piece, preferred_element_type=jnp.float32) for piece in pieces)
        )

    conv_sums = contract_all(
        (
            lax.all_gather(conv_b_w, "sp", axis=0, tiled=True),
            lax.all_gather(conv_c_w, "sp", axis=0, tiled=True),
            lax.all_gather(conv_x_w, "sp", axis=0, tiled=True),
        )
    )
    attn_sums = contract_all(
        (
            lax.all_gather(query_w, "sp", axis=0, tiled=True),
            lax.all_gather(key_w, "sp", axis=0, tiled=True),
            lax.all_gather(value_w, "sp", axis=0, tiled=True),
        )
    )
    sums = conv_sums + attn_sums
    gate_b, gate_c, conv_in, query, key, value = [
        (total * scale_rows).astype(jnp.bfloat16) for total in sums
    ]
    taps = conv_taps.shape[0]
    channels = conv_in.shape[1]
    conv_src = (gate_c.astype(jnp.float32) * conv_in.astype(jnp.float32)).astype(jnp.bfloat16)
    earlier = passed_along(conv_src[count - (taps - 1) :], "sp", 1)
    padded = jnp.concatenate([earlier, conv_src], axis=0)
    filtered = jnp.zeros((count, channels), jnp.float32)
    for tap in range(taps):
        filtered = filtered + conv_taps[tap][None, :] * padded[tap : tap + count].astype(
            jnp.float32
        )
    conv_out = (gate_b.astype(jnp.float32) * filtered).astype(jnp.bfloat16)
    heads_dev = gate_cache.shape[1]
    kv_dev = key.shape[1] // HD
    group = heads_dev // kv_dev
    half = count // 2
    sp_index = lax.axis_index("sp")
    own_start = sp_index * count
    scale = HD ** (-0.5)
    later_query = query[half:]
    later_start = own_start + half

    def prepare(q_rows, begin):
        heads_q = q_rows.reshape(half, kv_dev, group, HD)
        q_gate = lax.dynamic_slice_in_dim(gate_cache, begin, half, 0).T.reshape(
            kv_dev, group, half, 1
        )
        q_pos = begin + jnp.arange(half, dtype=jnp.int32)
        return (heads_q, q_gate, q_pos)

    sides = (prepare(query[:half], own_start), prepare(later_query, later_start))

    def absorb(carry, side, key_rows, value_rows, begin):
        heads_q, q_gate, q_pos = side
        run_max, run_sum, acc = carry
        width = key_rows.shape[0]
        key_heads = key_rows.reshape(width, kv_dev, HD)
        value_heads = value_rows.reshape(width, kv_dev, HD)
        score = (
            jnp.einsum("qgjd,kgd->gjqk", heads_q, key_heads, preferred_element_type=jnp.float32)
            * scale
        )
        key_gate = lax.dynamic_slice_in_dim(gate_cache, begin, width, 0).T.reshape(
            kv_dev, group, 1, width
        )
        score = score + q_gate - key_gate
        mask = (begin + jnp.arange(width, dtype=jnp.int32))[None, :] <= q_pos[:, None]
        score = jnp.where(mask, score, -1e30)
        new_max = jnp.maximum(run_max, jnp.max(score, axis=-1))
        weight = jnp.where(mask, jnp.exp(score - new_max[..., None]), 0.0)
        factor = jnp.exp(run_max - new_max)
        new_sum = run_sum * factor + jnp.sum(weight, axis=-1)
        product = jnp.einsum(
            "gjqk,kgd->gjqd",
            weight.astype(jnp.bfloat16),
            value_heads,
            preferred_element_type=jnp.float32,
        )
        return (new_max, new_sum, acc * factor[..., None] + product)

    def guarded(carry, side, key_rows, value_rows, begin):

        def visit_rows(state):
            return absorb(state, side, key_rows, value_rows, begin)

        def keep(state):
            return state

        return lax.cond(begin <= side[2][half - 1], visit_rows, keep, carry)

    def absorb_both(carry, key_rows, value_rows, begin):
        return (
            guarded(carry[0], sides[0], key_rows, value_rows, begin),
            guarded(carry[1], sides[1], key_rows, value_rows, begin),
        )

    def fresh():
        return (
            jnp.full((kv_dev, group, half), -1e30, jnp.float32),
            jnp.zeros((kv_dev, group, half), jnp.float32),
            jnp.zeros((kv_dev, group, half, HD), jnp.float32),
        )

    key_rows = lax.all_gather(key, "sp", axis=0, tiled=True)
    value_rows = lax.all_gather(value, "sp", axis=0, tiled=True)
    width = key_rows.shape[0]
    step = 512
    key_blocks = key_rows.reshape(width // step, step, key_rows.shape[1])
    value_blocks = value_rows.reshape(width // step, step, value_rows.shape[1])
    firsts = step * jnp.arange(width // step, dtype=jnp.int32)

    def visit(state, inputs):
        return (absorb_both(state, inputs[0], inputs[1], inputs[2]), None)

    result, _ = lax.scan(visit, (fresh(), fresh()), (key_blocks, value_blocks, firsts))

    def finish(state):
        run_max, run_sum, acc = state
        out = (
            (acc / run_sum[..., None])
            .transpose(2, 0, 1, 3)
            .reshape(half, heads_dev * HD)
            .astype(jnp.bfloat16)
        )
        lse = (run_max + jnp.log(run_sum)).transpose(2, 0, 1).reshape(half, heads_dev)
        return (out, lse)

    early_out, early_lse = finish(result[0])
    later_out, later_lse = finish(result[1])
    attn_out = jnp.concatenate([early_out, later_out], axis=0)
    log_total = jnp.concatenate([early_lse, later_lse], axis=0)
    term = jnp.dot(conv_out, out_conv_w, preferred_element_type=jnp.float32)
    mixed = lax.psum_scatter(
        (term + jnp.dot(attn_out, out_attn_w, preferred_element_type=jnp.float32)).astype(
            jnp.bfloat16
        ),
        "tp",
        scatter_dimension=0,
        tiled=True,
    )
    return (mixed, log_total)


def shape(dims, dtype=jnp.bfloat16):
    return jax.ShapeDtypeStruct(dims, dtype)


def run(kernel, where, operands, outs, scratch, flops, nbytes, mib, spec=VMEM):
    return pl.pallas_call(
        kernel,
        out_shape=outs,
        in_specs=[SMEM] + [spec] * len(operands),
        out_specs=jax.tree.map(lambda unused: VMEM, outs),
        scratch_shapes=scratch,
        cost_estimate=pl.CostEstimate(flops=flops, bytes_accessed=nbytes, transcendentals=0),
        compiler_params=pltpu.CompilerParams(vmem_limit_bytes=mib << 20),
    )(where, *operands)


def low_half(width):
    return lax.broadcasted_iota(jnp.int32, (1, width), 1) < width // 2


def pack_kernel(n, at, *rest):
    sources, rest = rest[:6], rest[6:]
    outs, held, sems = rest[:n], rest[n : n + 6], rest[n + 6]
    own, part = at[0], at[2]
    copies = [
        pltpu.make_async_copy(source, ref, sems.at[index])
        for index, (source, ref) in enumerate(zip(sources, held))
    ]
    for copy in copies:
        copy.start()
    for copy in copies:
        copy.wait()
    b_ref, c_ref, x_ref, q_ref, k_ref, v_ref = held

    def both(ref):
        turned = ref[...].astype(jnp.float32)
        return jnp.concatenate([turned, turned], axis=0).T

    key, value = both(k_ref), both(v_ref)
    low = low_half(LANES)
    for step in range(n):
        to = own ^ step
        tile = pl.ds(pl.multiple_of((to // 2) * LANES, LANES), LANES)
        odd = (to % 2) == 1

        def sides(ref):
            plain = ref[:, tile].astype(jnp.float32)
            return plain, pltpu.roll(plain, LANES // 2, 1)

        def lower(ref):
            plain, rolled = sides(ref)
            return jnp.where(odd, rolled, plain)

        def upper(ref):
            plain, rolled = sides(ref)
            return jnp.where(odd, plain, rolled)

        tiles = (
            jnp.where(low, lower(b_ref), upper(q_ref)),
            jnp.where(low, lower(c_ref), key),
            jnp.where(low, lower(x_ref), value),
        )
        for index, full in enumerate(tiles):
            columns = slice(index * LANES, (index + 1) * LANES)
            full = full.astype(jnp.bfloat16)
            out = outs[step]
            if step == 0:
                out[:, columns] = full
            else:
                half = out.shape[0]
                out[:, columns] = jnp.where(part == 0, full[:half], full[half:])


def order_kernel(n, at, conv_w, attn_w, out):
    own = at[0]
    for step in range(n):
        begin = pl.multiple_of((own ^ step) * HD, HD)
        out[step * LANES : step * LANES + HD, :] = conv_w[pl.ds(begin, HD), :]
        out[step * LANES + HD : (step + 1) * LANES, :] = attn_w[pl.ds(begin, HD), :]


def columns_of(ref, start, depth):
    return ref[:, pl.ds(pl.multiple_of(start, depth), depth)]


def norm_kernel(kinds, at, gain_ref, t0, t1, t2, t3, weight, *rest):
    pieces, (normed, scales, total) = rest[: len(kinds)], rest[len(kinds) :]
    own, column = at[0], at[1]
    gain = gain_ref[...]
    for index, ref in enumerate((t0, t1, t2, t3)):
        count = ref.shape[0]
        rows = pl.ds(pl.multiple_of((column ^ index) * count, count), count)
        xf = ref[...].astype(jnp.float32)
        scale = lax.rsqrt(jnp.mean(xf * xf, axis=-1, keepdims=True) + EPS)
        scales[rows, :] = jnp.broadcast_to(scale, (count, LANES))
        normed[rows, :] = (xf * gain).astype(jnp.bfloat16)
    depth = weight.shape[0]
    first = jnp.dot(
        columns_of(normed, own * depth, depth), weight[...], preferred_element_type=jnp.float32
    )
    if kinds:
        first = first + terms(at, normed, [(*kind, ref) for kind, ref in zip(kinds, pieces)])
    total[...] = first


def terms(at, normed, pieces):
    own, part = at[0], at[2]
    total = None
    for step, handed, ref in pieces:
        half = ref.shape[0]
        start = (own ^ step) * (2 * half) + ((1 - part) if handed else part) * half
        term = jnp.dot(
            columns_of(normed, start, half), ref[...], preferred_element_type=jnp.float32
        )
        total = term if total is None else total + term
    return total


def join_kernel(blocks, kinds, at, *rest):
    normed, totals = rest[:blocks], rest[blocks : 2 * blocks]
    pieces, outs = rest[2 * blocks : -blocks], rest[-blocks:]
    listed = [(*kind, ref) for kind, ref in zip(kinds, pieces)]
    for index in range(blocks):
        outs[index][...] = totals[index][...] + terms(at, normed[index], listed)


def mix_kernel(n, kinds, at, *rest):
    normed, totals, scales = rest[:n], rest[n : 2 * n], rest[2 * n : 3 * n]
    pieces, rest = rest[3 * n : 3 * n + len(kinds)], rest[3 * n + len(kinds) :]
    taps_ref, gate_ref = rest[:2]
    outs, (held, source, mixed, lse) = rest[2 : 2 + n], rest[2 + n :]
    own = at[0]
    count = normed[0].shape[0]
    rows_all = n * count
    listed = [(*kind, ref) for kind, ref in zip(kinds, pieces)]
    for step in range(n):
        begin = pl.multiple_of((own ^ step) * count, count)
        total = totals[step][...] + terms(at, normed[step], listed)
        held[pl.ds(begin, count), :] = (total * scales[step][:, :1]).astype(jnp.bfloat16)
    low = low_half(LANES)
    lead = source.shape[0] - rows_all
    source[:lead, :] = jnp.zeros((lead, LANES), jnp.float32)
    gated = held[:, LANES : 2 * LANES].astype(jnp.float32) * held[:, 2 * LANES :].astype(
        jnp.float32
    )
    source[lead:, :] = gated.astype(jnp.bfloat16).astype(jnp.float32)
    taps_n = taps_ref.shape[0]
    tile = pl.ds(pl.multiple_of((own // 2) * LANES, LANES), LANES)
    taps = taps_ref[:, tile]
    taps = jnp.where((own % 2) == 1, pltpu.roll(taps, LANES // 2, 1), taps)
    gate_row = gate_ref[pl.ds(own, 1), :]
    gate_column = jnp.broadcast_to(gate_row, (LANES, rows_all)).T
    scale = HD ** (-0.5)
    ahead = lax.broadcasted_iota(jnp.int32, (count, count), 0) >= lax.broadcasted_iota(
        jnp.int32, (count, count), 1
    )
    for block in range(n):
        first = block * count
        last = first + count
        filtered = jnp.zeros((count, LANES), jnp.float32)
        for tap in range(taps_n):
            begin = lead + first + tap - (taps_n - 1)
            filtered = filtered + taps[tap : tap + 1, :] * source[begin : begin + count, :]
        front = held[first:last, :LANES]
        conv = front.astype(jnp.float32) * filtered
        query = jnp.where(low, jnp.zeros_like(front), front)
        score = (
            lax.dot_general(
                query,
                held[:last, LANES : 2 * LANES],
                (((1,), (1,)), ((), ())),
                preferred_element_type=jnp.float32,
            )
            * scale
        )
        score = score + gate_column[first:last, :1] - gate_row[:, :last]
        edge = jnp.where(ahead, score[:, first:], -1e30)
        if block:
            before = score[:, :first]
            top = jnp.maximum(
                jnp.max(before, axis=-1, keepdims=True), jnp.max(edge, axis=-1, keepdims=True)
            )
            weight = jnp.concatenate([jnp.exp(before - top), jnp.exp(edge - top)], axis=1)
        else:
            top = jnp.max(edge, axis=-1, keepdims=True)
            weight = jnp.exp(edge - top)
        total = jnp.sum(weight, axis=-1, keepdims=True)
        product = jnp.dot(
            weight.astype(jnp.bfloat16),
            held[:last, 2 * LANES :],
            preferred_element_type=jnp.float32,
        )
        mixed[first:last, :] = jnp.where(low, conv, product / total).astype(jnp.bfloat16)
        lse[block : block + 1, :] = jnp.broadcast_to(top + jnp.log(total), (count, LANES)).T[:1, :]
    for step in range(n):
        to = own ^ step
        outs[step][:count, :] = mixed[pl.ds(pl.multiple_of(to * count, count), count), :]
        left, lines = lse[pl.ds(to, 1), :], []
        for _ in range(PIECES):
            piece = left.astype(jnp.bfloat16).astype(jnp.float32)
            lines += [piece[:, at : at + LANES] for at in range(0, count, LANES)]
            left = left - piece
        lines.append(jnp.zeros((outs[step].shape[0] - count - len(lines), LANES), jnp.float32))
        outs[step][count:, :] = jnp.concatenate(lines, axis=0).astype(jnp.bfloat16)


def out_kernel(n, at, *rest):
    parts, weights = rest[: 2 * n], rest[2 * n : 2 * n + 2]
    far, near, logs, joined = rest[2 * n + 2 :]
    own, column = at[0], at[1]
    count, width = far.shape
    positions = logs.shape[1]
    lines = positions // LANES
    for step in range(n):
        tail = parts[step][positions:, :].astype(jnp.float32)
        row = []
        for line in range(lines):
            value = tail[line : line + 1]
            for piece in range(1, PIECES):
                place = piece * lines + line
                value = value + tail[place : place + 1]
            row.append(value)
        logs[pl.ds(own ^ step, 1), :] = jnp.concatenate(row, axis=1)
    for place, row in enumerate((column ^ 2, column)):
        begin = pl.multiple_of(row * count, count)
        for index, ref in enumerate(parts):
            joined[
                place * count : (place + 1) * count, index * LANES : (index + 1) * LANES
            ] = ref[pl.ds(begin, count), :]
    tile = 2 * LANES
    for begin in range(0, width, tile):
        columns = slice(begin, begin + tile)
        total = None
        for index, ref in enumerate(weights):
            term = jnp.dot(
                joined[:, index * n * LANES : (index + 1) * n * LANES],
                ref[:, columns],
                preferred_element_type=jnp.float32,
            )
            total = term if total is None else total + term
        far[:, columns] = total[:count].astype(jnp.bfloat16)
        near[:, columns] = total[count:]


def sum_kernel(near, far, out):
    out[...] = (near[...] + far[...].astype(jnp.float32)).astype(jnp.bfloat16)


def pick_kernel(n, at, inner, outer, out):
    own = at[0]
    end = (own == 0) | (own == n - 1)

    @pl.when(end)
    def take_outer():
        out[...] = outer[...]

    @pl.when(jnp.logical_not(end))
    def take_inner():
        out[...] = inner[...]


def by_columns(
    tokens,
    norm_gain,
    conv_b_w,
    conv_c_w,
    conv_x_w,
    query_w,
    key_w,
    value_w,
    conv_taps,
    gate_cache,
    out_conv_w,
    out_attn_w,
):
    n, n_tp = lax.axis_size("sp"), lax.axis_size("tp")
    where = jnp.stack([lax.axis_index("sp"), lax.axis_index("tp"), lax.axis_index("grp")])
    where = where.astype(jnp.int32)
    swap = lambda bit: [(i, i ^ bit) for i in range(n)]
    last = n - 1
    outward = [(n // 2, last), (n // 2 - 1, 0)]
    inward = [(0, n // 2), (last, n // 2 - 1)]
    middle = [(n // 2 - 1, n // 2), (n // 2, n // 2 - 1)]
    m, d = tokens.shape
    depth, width = conv_b_w.shape
    packed = 3 * LANES
    half = depth // 2
    count = m * n_tp
    rows = n * count
    gain = norm_gain.reshape(1, d)
    z1 = lax.ppermute(tokens, "sp", swap(1))
    z3a = lax.ppermute(tokens, "sp", middle)
    z2a = lax.ppermute(tokens, "sp", inward)
    own_w, *sends = run(
        functools.partial(pack_kernel, n),
        where,
        (conv_b_w, conv_c_w, conv_x_w, query_w, key_w.T, value_w.T),
        [shape((depth, packed))] + [shape((half, packed))] * (n - 1),
        [pltpu.VMEM((depth, width), jnp.bfloat16)] * 4
        + [pltpu.VMEM((key_w.shape[1], depth), jnp.bfloat16)] * 2
        + [pltpu.SemaphoreType.DMA((6,))],
        depth * packed * n,
        6 * depth * width,
        PACK_MIB,
        pl.BlockSpec(memory_space=pltpu.HBM),
    )
    came = {k: lax.ppermute(sends[k - 1], "sp", swap(k)) for k in range(1, n)}
    given = {k: lax.ppermute(came[k], "grp", [(0, 1), (1, 0)]) for k in range(1, n)}
    z2b = lax.ppermute(z3a, "sp", outward)
    z3b = lax.ppermute(z2a, "sp", outward)

    def pick(inner, outer):
        return run(
            functools.partial(pick_kernel, n),
            where,
            (inner, outer),
            shape((m, d)),
            [],
            0,
            6 * m * d,
            2,
        )

    z2 = pick(z2a, z2b)
    z3 = pick(z3a, z3b)
    out_w = run(
        functools.partial(order_kernel, n),
        where,
        (out_conv_w, out_attn_w),
        shape((n * LANES, d)),
        [],
        0,
        4 * n * LANES * d,
        4,
    )
    out_w_other = lax.ppermute(out_w, "tp", swap(1))
    piece = lambda kind: (given if kind[1] else came)[kind[0]]
    normed, scales, totals = [], [], []
    for k, mine in enumerate((tokens, z1, z2, z3)):
        kinds = EARLY if k == n - 1 else ()
        over = lax.ppermute(mine, "tp", swap(2))
        side = lax.ppermute(mine, "tp", swap(1))
        cross = lax.ppermute(over, "tp", swap(1))
        results = run(
            functools.partial(norm_kernel, kinds),
            where,
            (gain, mine, side, over, cross, own_w, *(piece(kind) for kind in kinds)),
            [
                shape((count, d)),
                shape((count, LANES), jnp.float32),
                shape((count, packed), jnp.float32),
            ],
            [],
            2 * count * (depth + half * len(kinds)) * packed,
            4 * count * d,
            4,
        )
        normed.append(results[0])
        scales.append(results[1])
        totals.append(results[2])
    blocks = n - 1
    joined = run(
        functools.partial(join_kernel, blocks, EARLY),
        where,
        (*normed[:blocks], *totals[:blocks], *(piece(kind) for kind in EARLY)),
        [shape((count, packed), jnp.float32)] * blocks,
        [],
        2 * blocks * count * half * len(EARLY) * packed,
        8 * rows * packed,
        4,
    )
    totals = [*joined, totals[-1]]
    late = LATE
    extra = -(-PIECES * count // (SUBLANES * LANES)) * SUBLANES
    results = run(
        functools.partial(mix_kernel, n, late),
        where,
        (
            *normed,
            *totals,
            *scales,
            *(piece(kind) for kind in late),
            conv_taps,
            gate_cache.T,
        ),
        [shape((count + extra, LANES))] * n,
        [
            pltpu.VMEM((rows, packed), jnp.bfloat16),
            pltpu.VMEM((rows + 8, LANES), jnp.float32),
            pltpu.VMEM((rows, LANES), jnp.bfloat16),
            pltpu.VMEM((n, count), jnp.float32),
        ],
        4 * rows * rows * LANES,
        2 * rows * packed,
        12,
    )
    parts = [results[0]] + [lax.ppermute(results[k], "sp", swap(k)) for k in range(1, n)]

    other = [lax.ppermute(part, "tp", swap(1)) for part in parts]
    far, near, log_rows = run(
        functools.partial(out_kernel, n),
        where,
        (*parts, *other, out_w, out_w_other),
        [shape((m, d)), shape((m, d), jnp.float32), shape((n, count), jnp.float32)],
        [pltpu.VMEM((2 * m, 2 * n * LANES), jnp.bfloat16)],
        8 * m * n * LANES * d,
        4 * n * LANES * d,
        8,
    )
    came_far = lax.ppermute(far, "tp", swap(2))
    mixed = pl.pallas_call(
        sum_kernel,
        out_shape=shape((m, d)),
        in_specs=[VMEM] * 2,
        out_specs=VMEM,
        name="total",
        cost_estimate=pl.CostEstimate(flops=4 * m * d, bytes_accessed=10 * m * d, transcendentals=0),
        compiler_params=pltpu.CompilerParams(vmem_limit_bytes=4 << 20),
    )(near, came_far)
    return (mixed, log_rows.T)


PIECES = 3
PACK_MIB = 58
SUBLANES = 16
EARLY = ((1, False), (3, False), (2, False), (1, True))
LATE = ((3, True), (2, True))


def on_device(*operands):
    tokens, key_w, gate_cache = operands[0], operands[6], operands[9]
    n, n_tp, n_grp = (lax.axis_size(name) for name in ("sp", "tp", "grp"))
    channels = operands[2].shape[1]
    heads = gate_cache.shape[1]
    fits = (
        n == heads == 4
        and n_tp == 4
        and n_grp == 2
        and key_w.shape[1] == HD
        and channels == n * HD
        and 2 * HD == LANES
        and gate_cache.shape[0] == n * n_tp * tokens.shape[0]
    )
    return (by_columns if fits else by_rows)(*operands)


def solution(mesh):
    placed = (
        P(("grp", "sp", "tp"), None),
        P(),
        P("sp", "tp"),
        P("sp", "tp"),
        P("sp", "tp"),
        P("sp", "tp"),
        P("sp", "tp"),
        P("sp", "tp"),
        P(None, "tp"),
        P("grp", "tp"),
        P("tp", None),
        P("tp", None),
    )
    return jax.shard_map(
        on_device,
        mesh=mesh,
        in_specs=placed,
        out_specs=(P(("grp", "sp", "tp"), None), P(("grp", "sp"), "tp")),
        check_vma=False,
    )
```

```python
import functools

import jax
import jax.numpy as jnp
from jax import lax
from jax.experimental import pallas as pl
from jax.experimental.pallas import tpu as pltpu
from jax.sharding import PartitionSpec as P

HD = 64
LANES = 128
EPS = 1e-05
VMEM = pl.BlockSpec(memory_space=pltpu.VMEM)
SMEM = pl.BlockSpec(memory_space=pltpu.SMEM)


def passed_along(value, axis, by):
    count = lax.axis_size(axis)
    pairs = [(i, i + by) for i in range(count) if 0 <= i + by < count]
    return lax.ppermute(value, axis, pairs)


def by_rows(
    tokens,
    norm_gain,
    conv_b_w,
    conv_c_w,
    conv_x_w,
    query_w,
    key_w,
    value_w,
    conv_taps,
    gate_cache,
    out_conv_w,
    out_attn_w,
):
    rows = lax.all_gather(tokens, "tp", axis=0, tiled=True)
    count = rows.shape[0]
    xf = rows.astype(jnp.float32)
    scale_rows = lax.rsqrt(jnp.mean(xf * xf, axis=-1, keepdims=True) + 1e-05)
    normed = (xf * norm_gain).astype(jnp.bfloat16)

    def contract_all(pieces):
        return tuple(
            (jnp.dot(normed, piece, preferred_element_type=jnp.float32) for piece in pieces)
        )

    conv_sums = contract_all(
        (
            lax.all_gather(conv_b_w, "sp", axis=0, tiled=True),
            lax.all_gather(conv_c_w, "sp", axis=0, tiled=True),
            lax.all_gather(conv_x_w, "sp", axis=0, tiled=True),
        )
    )
    attn_sums = contract_all(
        (
            lax.all_gather(query_w, "sp", axis=0, tiled=True),
            lax.all_gather(key_w, "sp", axis=0, tiled=True),
            lax.all_gather(value_w, "sp", axis=0, tiled=True),
        )
    )
    sums = conv_sums + attn_sums
    gate_b, gate_c, conv_in, query, key, value = [
        (total * scale_rows).astype(jnp.bfloat16) for total in sums
    ]
    taps = conv_taps.shape[0]
    channels = conv_in.shape[1]
    conv_src = (gate_c.astype(jnp.float32) * conv_in.astype(jnp.float32)).astype(jnp.bfloat16)
    earlier = passed_along(conv_src[count - (taps - 1) :], "sp", 1)
    padded = jnp.concatenate([earlier, conv_src], axis=0)
    filtered = jnp.zeros((count, channels), jnp.float32)
    for tap in range(taps):
        filtered = filtered + conv_taps[tap][None, :] * padded[tap : tap + count].astype(
            jnp.float32
        )
    conv_out = (gate_b.astype(jnp.float32) * filtered).astype(jnp.bfloat16)
    heads_dev = gate_cache.shape[1]
    kv_dev = key.shape[1] // HD
    group = heads_dev // kv_dev
    half = count // 2
    sp_index = lax.axis_index("sp")
    own_start = sp_index * count
    scale = HD ** (-0.5)
    later_query = query[half:]
    later_start = own_start + half

    def prepare(q_rows, begin):
        heads_q = q_rows.reshape(half, kv_dev, group, HD)
        q_gate = lax.dynamic_slice_in_dim(gate_cache, begin, half, 0).T.reshape(
            kv_dev, group, half, 1
        )
        q_pos = begin + jnp.arange(half, dtype=jnp.int32)
        return (heads_q, q_gate, q_pos)

    sides = (prepare(query[:half], own_start), prepare(later_query, later_start))

    def absorb(carry, side, key_rows, value_rows, begin):
        heads_q, q_gate, q_pos = side
        run_max, run_sum, acc = carry
        width = key_rows.shape[0]
        key_heads = key_rows.reshape(width, kv_dev, HD)
        value_heads = value_rows.reshape(width, kv_dev, HD)
        score = (
            jnp.einsum("qgjd,kgd->gjqk", heads_q, key_heads, preferred_element_type=jnp.float32)
            * scale
        )
        key_gate = lax.dynamic_slice_in_dim(gate_cache, begin, width, 0).T.reshape(
            kv_dev, group, 1, width
        )
        score = score + q_gate - key_gate
        mask = (begin + jnp.arange(width, dtype=jnp.int32))[None, :] <= q_pos[:, None]
        score = jnp.where(mask, score, -1e30)
        new_max = jnp.maximum(run_max, jnp.max(score, axis=-1))
        weight = jnp.where(mask, jnp.exp(score - new_max[..., None]), 0.0)
        factor = jnp.exp(run_max - new_max)
        new_sum = run_sum * factor + jnp.sum(weight, axis=-1)
        product = jnp.einsum(
            "gjqk,kgd->gjqd",
            weight.astype(jnp.bfloat16),
            value_heads,
            preferred_element_type=jnp.float32,
        )
        return (new_max, new_sum, acc * factor[..., None] + product)

    def guarded(carry, side, key_rows, value_rows, begin):

        def visit_rows(state):
            return absorb(state, side, key_rows, value_rows, begin)

        def keep(state):
            return state

        return lax.cond(begin <= side[2][half - 1], visit_rows, keep, carry)

    def absorb_both(carry, key_rows, value_rows, begin):
        return (
            guarded(carry[0], sides[0], key_rows, value_rows, begin),
            guarded(carry[1], sides[1], key_rows, value_rows, begin),
        )

    def fresh():
        return (
            jnp.full((kv_dev, group, half), -1e30, jnp.float32),
            jnp.zeros((kv_dev, group, half), jnp.float32),
            jnp.zeros((kv_dev, group, half, HD), jnp.float32),
        )

    key_rows = lax.all_gather(key, "sp", axis=0, tiled=True)
    value_rows = lax.all_gather(value, "sp", axis=0, tiled=True)
    width = key_rows.shape[0]
    step = 512
    key_blocks = key_rows.reshape(width // step, step, key_rows.shape[1])
    value_blocks = value_rows.reshape(width // step, step, value_rows.shape[1])
    firsts = step * jnp.arange(width // step, dtype=jnp.int32)

    def visit(state, inputs):
        return (absorb_both(state, inputs[0], inputs[1], inputs[2]), None)

    result, _ = lax.scan(visit, (fresh(), fresh()), (key_blocks, value_blocks, firsts))

    def finish(state):
        run_max, run_sum, acc = state
        out = (
            (acc / run_sum[..., None])
            .transpose(2, 0, 1, 3)
            .reshape(half, heads_dev * HD)
            .astype(jnp.bfloat16)
        )
        lse = (run_max + jnp.log(run_sum)).transpose(2, 0, 1).reshape(half, heads_dev)
        return (out, lse)

    early_out, early_lse = finish(result[0])
    later_out, later_lse = finish(result[1])
    attn_out = jnp.concatenate([early_out, later_out], axis=0)
    log_total = jnp.concatenate([early_lse, later_lse], axis=0)
    term = jnp.dot(conv_out, out_conv_w, preferred_element_type=jnp.float32)
    mixed = lax.psum_scatter(
        (term + jnp.dot(attn_out, out_attn_w, preferred_element_type=jnp.float32)).astype(
            jnp.bfloat16
        ),
        "tp",
        scatter_dimension=0,
        tiled=True,
    )
    return (mixed, log_total)


def shape(dims, dtype=jnp.bfloat16):
    return jax.ShapeDtypeStruct(dims, dtype)


def run(kernel, operands, outs, scratch, flops, nbytes, mib, spec=VMEM):
    def placed(*refs):
        kernel(tuple(lax.axis_index(axis) for axis in ("sp", "tp", "grp")), *refs)

    return pl.pallas_call(
        placed,
        out_shape=outs,
        in_specs=[spec] * len(operands),
        out_specs=jax.tree.map(lambda unused: VMEM, outs),
        scratch_shapes=scratch,
        cost_estimate=pl.CostEstimate(flops=flops, bytes_accessed=nbytes, transcendentals=0),
        compiler_params=pltpu.CompilerParams(vmem_limit_bytes=mib << 20),
    )(*operands)


def low_half(width):
    return lax.broadcasted_iota(jnp.int32, (1, width), 1) < width // 2


def pack_kernel(n, at, *rest):
    sources, rest = rest[:6], rest[6:]
    outs, held, sems = rest[:n], rest[n : n + 6], rest[n + 6]
    own, part = at[0], at[2]
    copies = [
        pltpu.make_async_copy(source, ref, sems.at[index])
        for index, (source, ref) in enumerate(zip(sources, held))
    ]
    for copy in copies:
        copy.start()
    for copy in copies:
        copy.wait()
    b_ref, c_ref, x_ref, q_ref, k_ref, v_ref = held

    def both(ref):
        turned = ref[...].astype(jnp.float32)
        return jnp.concatenate([turned, turned], axis=0).T

    key, value = both(k_ref), both(v_ref)
    low = low_half(LANES)
    for step in range(n):
        to = own ^ step
        tile = pl.ds(pl.multiple_of((to // 2) * LANES, LANES), LANES)
        odd = (to % 2) == 1

        def sides(ref):
            plain = ref[:, tile].astype(jnp.float32)
            return plain, pltpu.roll(plain, LANES // 2, 1)

        def lower(ref):
            plain, rolled = sides(ref)
            return jnp.where(odd, rolled, plain)

        def upper(ref):
            plain, rolled = sides(ref)
            return jnp.where(odd, plain, rolled)

        tiles = (
            jnp.where(low, lower(b_ref), upper(q_ref)),
            jnp.where(low, lower(c_ref), key),
            jnp.where(low, lower(x_ref), value),
        )
        for index, full in enumerate(tiles):
            columns = slice(index * LANES, (index + 1) * LANES)
            full = full.astype(jnp.bfloat16)
            out = outs[step]
            if step == 0:
                out[:, columns] = full
            else:
                half = out.shape[0]
                out[:, columns] = jnp.where(part == 0, full[:half], full[half:])


def order_kernel(n, at, conv_w, attn_w, out):
    own = at[0]
    for step in range(n):
        begin = pl.multiple_of((own ^ step) * HD, HD)
        out[step * LANES : step * LANES + HD, :] = conv_w[pl.ds(begin, HD), :]
        out[step * LANES + HD : (step + 1) * LANES, :] = attn_w[pl.ds(begin, HD), :]


def columns_of(ref, start, depth):
    return ref[:, pl.ds(pl.multiple_of(start, depth), depth)]


def norm_kernel(kinds, at, gain_ref, t0, t1, t2, t3, weight, *rest):
    pieces, (normed, scales, total) = rest[: len(kinds)], rest[len(kinds) :]
    own, column = at[0], at[1]
    gain = gain_ref[...]
    for index, ref in enumerate((t0, t1, t2, t3)):
        count = ref.shape[0]
        rows = pl.ds(pl.multiple_of((column ^ index) * count, count), count)
        xf = ref[...].astype(jnp.float32)
        scale = lax.rsqrt(jnp.mean(xf * xf, axis=-1, keepdims=True) + EPS)
        scales[rows, :] = jnp.broadcast_to(scale, (count, LANES))
        normed[rows, :] = (xf * gain).astype(jnp.bfloat16)
    depth = weight.shape[0]
    first = jnp.dot(
        columns_of(normed, own * depth, depth), weight[...], preferred_element_type=jnp.float32
    )
    if kinds:
        first = first + terms(at, normed, [(*kind, ref) for kind, ref in zip(kinds, pieces)])
    total[...] = first


def terms(at, normed, pieces):
    own, part = at[0], at[2]
    total = None
    for step, handed, ref in pieces:
        half = ref.shape[0]
        start = (own ^ step) * (2 * half) + ((1 - part) if handed else part) * half
        term = jnp.dot(
            columns_of(normed, start, half), ref[...], preferred_element_type=jnp.float32
        )
        total = term if total is None else total + term
    return total


def join_kernel(blocks, kinds, at, *rest):
    normed, totals = rest[:blocks], rest[blocks : 2 * blocks]
    pieces, outs = rest[2 * blocks : -blocks], rest[-blocks:]
    listed = [(*kind, ref) for kind, ref in zip(kinds, pieces)]
    for index in range(blocks):
        outs[index][...] = totals[index][...] + terms(at, normed[index], listed)


def mix_kernel(n, kinds, at, *rest):
    normed, totals, scales = rest[:n], rest[n : 2 * n], rest[2 * n : 3 * n]
    pieces, rest = rest[3 * n : 3 * n + len(kinds)], rest[3 * n + len(kinds) :]
    taps_ref, gate_ref = rest[:2]
    outs, (held, source, mixed, lse) = rest[2 : 2 + n], rest[2 + n :]
    own = at[0]
    count = normed[0].shape[0]
    rows_all = n * count
    listed = [(*kind, ref) for kind, ref in zip(kinds, pieces)]
    for step in range(n):
        begin = pl.multiple_of((own ^ step) * count, count)
        total = totals[step][...] + terms(at, normed[step], listed)
        held[pl.ds(begin, count), :] = (total * scales[step][:, :1]).astype(jnp.bfloat16)
    low = low_half(LANES)
    lead = source.shape[0] - rows_all
    source[:lead, :] = jnp.zeros((lead, LANES), jnp.float32)
    gated = held[:, LANES : 2 * LANES].astype(jnp.float32) * held[:, 2 * LANES :].astype(
        jnp.float32
    )
    source[lead:, :] = gated.astype(jnp.bfloat16).astype(jnp.float32)
    taps_n = taps_ref.shape[0]
    tile = pl.ds(pl.multiple_of((own // 2) * LANES, LANES), LANES)
    taps = taps_ref[:, tile]
    taps = jnp.where((own % 2) == 1, pltpu.roll(taps, LANES // 2, 1), taps)
    gate_row = gate_ref[pl.ds(own, 1), :]
    scale = HD ** (-0.5)
    ahead = lax.broadcasted_iota(jnp.int32, (count, count), 0) >= lax.broadcasted_iota(
        jnp.int32, (count, count), 1
    )
    for block in range(n):
        first = block * count
        last = first + count
        filtered = jnp.zeros((count, LANES), jnp.float32)
        for tap in range(taps_n):
            begin = lead + first + tap - (taps_n - 1)
            filtered = filtered + taps[tap : tap + 1, :] * source[begin : begin + count, :]
        front = held[first:last, :LANES]
        conv = front.astype(jnp.float32) * filtered
        query = jnp.where(low, 0.0, front.astype(jnp.float32) * scale).astype(jnp.bfloat16)
        score = lax.dot_general(
            query,
            held[:last, LANES : 2 * LANES],
            (((1,), (1,)), ((), ())),
            preferred_element_type=jnp.float32,
        )
        score = score - gate_row[:, :last]
        edge = jnp.where(ahead, score[:, first:], -1e30)
        if block:
            before = score[:, :first]
            top = jnp.maximum(
                jnp.max(before, axis=-1, keepdims=True), jnp.max(edge, axis=-1, keepdims=True)
            )
            weight = jnp.concatenate([jnp.exp(before - top), jnp.exp(edge - top)], axis=1)
        else:
            top = jnp.max(edge, axis=-1, keepdims=True)
            weight = jnp.exp(edge - top)
        total = jnp.sum(weight, axis=-1, keepdims=True)
        product = jnp.dot(
            weight.astype(jnp.bfloat16),
            held[:last, 2 * LANES :],
            preferred_element_type=jnp.float32,
        )
        mixed[first:last, :] = jnp.where(low, conv, product / total).astype(jnp.bfloat16)
        lse[block : block + 1, :] = (
            jnp.broadcast_to(top + jnp.log(total), (count, LANES)).T[:1, :]
            + gate_row[:, first:last]
        )
    for step in range(n):
        to = own ^ step
        outs[step][:count, :] = mixed[pl.ds(pl.multiple_of(to * count, count), count), :]
        left, lines = lse[pl.ds(to, 1), :], []
        for _ in range(PIECES):
            piece = left.astype(jnp.bfloat16).astype(jnp.float32)
            lines += [piece[:, at : at + LANES] for at in range(0, count, LANES)]
            left = left - piece
        lines.append(jnp.zeros((outs[step].shape[0] - count - len(lines), LANES), jnp.float32))
        outs[step][count:, :] = jnp.concatenate(lines, axis=0).astype(jnp.bfloat16)


def out_kernel(n, at, *rest):
    parts, weights = rest[: 2 * n], rest[2 * n : 2 * n + 2]
    far, near, logs, joined = rest[2 * n + 2 :]
    own, column = at[0], at[1]
    count, width = far.shape
    positions = logs.shape[1]
    lines = positions // LANES
    for step in range(n):
        tail = parts[step][positions:, :].astype(jnp.float32)
        row = []
        for line in range(lines):
            value = tail[line : line + 1]
            for piece in range(1, PIECES):
                place = piece * lines + line
                value = value + tail[place : place + 1]
            row.append(value)
        logs[pl.ds(own ^ step, 1), :] = jnp.concatenate(row, axis=1)
    for place, row in enumerate((column ^ 2, column)):
        begin = pl.multiple_of(row * count, count)
        for index, ref in enumerate(parts):
            joined[
                place * count : (place + 1) * count, index * LANES : (index + 1) * LANES
            ] = ref[pl.ds(begin, count), :]
    tile = 2 * LANES
    for begin in range(0, width, tile):
        columns = slice(begin, begin + tile)
        total = None
        for index, ref in enumerate(weights):
            term = jnp.dot(
                joined[:, index * n * LANES : (index + 1) * n * LANES],
                ref[:, columns],
                preferred_element_type=jnp.float32,
            )
            total = term if total is None else total + term
        far[:, columns] = total[:count].astype(jnp.bfloat16)
        near[:, columns] = total[count:]


def sum_kernel(near, far, out):
    out[...] = (near[...] + far[...].astype(jnp.float32)).astype(jnp.bfloat16)


def pick_kernel(n, at, inner, outer, out):
    own = at[0]
    end = (own == 0) | (own == n - 1)

    @pl.when(end)
    def take_outer():
        out[...] = outer[...]

    @pl.when(jnp.logical_not(end))
    def take_inner():
        out[...] = inner[...]


def by_columns(
    tokens,
    norm_gain,
    conv_b_w,
    conv_c_w,
    conv_x_w,
    query_w,
    key_w,
    value_w,
    conv_taps,
    gate_cache,
    out_conv_w,
    out_attn_w,
):
    n, n_tp = lax.axis_size("sp"), lax.axis_size("tp")
    swap = lambda bit: [(i, i ^ bit) for i in range(n)]
    last = n - 1
    outward = [(n // 2, last), (n // 2 - 1, 0)]
    inward = [(0, n // 2), (last, n // 2 - 1)]
    middle = [(n // 2 - 1, n // 2), (n // 2, n // 2 - 1)]
    m, d = tokens.shape
    depth, width = conv_b_w.shape
    packed = 3 * LANES
    half = depth // 2
    count = m * n_tp
    rows = n * count
    gain = norm_gain.reshape(1, d)
    z1 = lax.ppermute(tokens, "sp", swap(1))
    z3a = lax.ppermute(tokens, "sp", middle)
    z2a = lax.ppermute(tokens, "sp", inward)
    own_w, *sends = run(
        functools.partial(pack_kernel, n),
        (conv_b_w, conv_c_w, conv_x_w, query_w, key_w.T, value_w.T),
        [shape((depth, packed))] + [shape((half, packed))] * (n - 1),
        [pltpu.VMEM((depth, width), jnp.bfloat16)] * 4
        + [pltpu.VMEM((key_w.shape[1], depth), jnp.bfloat16)] * 2
        + [pltpu.SemaphoreType.DMA((6,))],
        depth * packed * n,
        6 * depth * width,
        PACK_MIB,
        pl.BlockSpec(memory_space=pltpu.HBM),
    )
    came = {k: lax.ppermute(sends[k - 1], "sp", swap(k)) for k in range(1, n)}
    given = {k: lax.ppermute(came[k], "grp", [(0, 1), (1, 0)]) for k in range(1, n)}
    z2b = lax.ppermute(z3a, "sp", outward)
    z3b = lax.ppermute(z2a, "sp", outward)

    def pick(inner, outer):
        return run(
            functools.partial(pick_kernel, n), (inner, outer), shape((m, d)), [], 0, 6 * m * d, 2
        )

    z2 = pick(z2a, z2b)
    z3 = pick(z3a, z3b)
    out_w = run(
        functools.partial(order_kernel, n),
        (out_conv_w, out_attn_w),
        shape((n * LANES, d)),
        [],
        0,
        4 * n * LANES * d,
        4,
    )
    out_w_other = lax.ppermute(out_w, "tp", swap(1))
    piece = lambda kind: (given if kind[1] else came)[kind[0]]
    normed, scales, totals = [], [], []
    for k, mine in enumerate((tokens, z1, z2, z3)):
        kinds = EARLY if k == n - 1 else ()
        over = lax.ppermute(mine, "tp", swap(2))
        side = lax.ppermute(mine, "tp", swap(1))
        cross = lax.ppermute(over, "tp", swap(1))
        results = run(
            functools.partial(norm_kernel, kinds),
            (gain, mine, side, over, cross, own_w, *(piece(kind) for kind in kinds)),
            [
                shape((count, d)),
                shape((count, LANES), jnp.float32),
                shape((count, packed), jnp.float32),
            ],
            [],
            2 * count * (depth + half * len(kinds)) * packed,
            4 * count * d,
            4,
        )
        normed.append(results[0])
        scales.append(results[1])
        totals.append(results[2])
    blocks = n - 1
    joined = run(
        functools.partial(join_kernel, blocks, EARLY),
        (*normed[:blocks], *totals[:blocks], *(piece(kind) for kind in EARLY)),
        [shape((count, packed), jnp.float32)] * blocks,
        [],
        2 * blocks * count * half * len(EARLY) * packed,
        8 * rows * packed,
        4,
    )
    totals = [*joined, totals[-1]]
    late = LATE
    extra = -(-PIECES * count // (SUBLANES * LANES)) * SUBLANES
    results = run(
        functools.partial(mix_kernel, n, late),
        (
            *normed,
            *totals,
            *scales,
            *(piece(kind) for kind in late),
            conv_taps,
            gate_cache.T,
        ),
        [shape((count + extra, LANES))] * n,
        [
            pltpu.VMEM((rows, packed), jnp.bfloat16),
            pltpu.VMEM((rows + 8, LANES), jnp.float32),
            pltpu.VMEM((rows, LANES), jnp.bfloat16),
            pltpu.VMEM((n, count), jnp.float32),
        ],
        4 * rows * rows * LANES,
        2 * rows * packed,
        12,
    )
    parts = [results[0]] + [lax.ppermute(results[k], "sp", swap(k)) for k in range(1, n)]

    other = [lax.ppermute(part, "tp", swap(1)) for part in parts]
    far, near, log_rows = run(
        functools.partial(out_kernel, n),
        (*parts, *other, out_w, out_w_other),
        [shape((m, d)), shape((m, d), jnp.float32), shape((n, count), jnp.float32)],
        [pltpu.VMEM((2 * m, 2 * n * LANES), jnp.bfloat16)],
        8 * m * n * LANES * d,
        4 * n * LANES * d,
        8,
    )
    came_far = lax.ppermute(far, "tp", swap(2))
    mixed = pl.pallas_call(
        sum_kernel,
        out_shape=shape((m, d)),
        in_specs=[VMEM] * 2,
        out_specs=VMEM,
        name="total",
        cost_estimate=pl.CostEstimate(flops=4 * m * d, bytes_accessed=10 * m * d, transcendentals=0),
        compiler_params=pltpu.CompilerParams(vmem_limit_bytes=4 << 20),
    )(near, came_far)
    return (mixed, log_rows.T)


PIECES = 3
PACK_MIB = 58
SUBLANES = 16
EARLY = ((1, False), (3, False), (2, False), (1, True))
LATE = ((3, True), (2, True))


def on_device(*operands):
    tokens, key_w, gate_cache = operands[0], operands[6], operands[9]
    n, n_tp, n_grp = (lax.axis_size(name) for name in ("sp", "tp", "grp"))
    channels = operands[2].shape[1]
    heads = gate_cache.shape[1]
    fits = (
        n == heads == 4
        and n_tp == 4
        and n_grp == 2
        and key_w.shape[1] == HD
        and channels == n * HD
        and 2 * HD == LANES
        and gate_cache.shape[0] == n * n_tp * tokens.shape[0]
    )
    return (by_columns if fits else by_rows)(*operands)


def solution(mesh):
    placed = (
        P(("grp", "sp", "tp"), None),
        P(),
        P("sp", "tp"),
        P("sp", "tp"),
        P("sp", "tp"),
        P("sp", "tp"),
        P("sp", "tp"),
        P("sp", "tp"),
        P(None, "tp"),
        P("grp", "tp"),
        P("tp", None),
        P("tp", None),
    )
    return jax.shard_map(
        on_device,
        mesh=mesh,
        in_specs=placed,
        out_specs=(P(("grp", "sp", "tp"), None), P(("grp", "sp"), "tp")),
        check_vma=False,
    )
```

```python
import functools

import jax
import jax.numpy as jnp
from jax import lax
from jax.experimental import pallas as pl
from jax.experimental.pallas import tpu as pltpu
from jax.sharding import PartitionSpec as P

HD = 64
LANES = 128
EPS = 1e-05
VMEM = pl.BlockSpec(memory_space=pltpu.VMEM)
SMEM = pl.BlockSpec(memory_space=pltpu.SMEM)


def passed_along(value, axis, by):
    count = lax.axis_size(axis)
    pairs = [(i, i + by) for i in range(count) if 0 <= i + by < count]
    return lax.ppermute(value, axis, pairs)


def by_rows(
    tokens,
    norm_gain,
    conv_b_w,
    conv_c_w,
    conv_x_w,
    query_w,
    key_w,
    value_w,
    conv_taps,
    gate_cache,
    out_conv_w,
    out_attn_w,
):
    rows = lax.all_gather(tokens, "tp", axis=0, tiled=True)
    count = rows.shape[0]
    xf = rows.astype(jnp.float32)
    scale_rows = lax.rsqrt(jnp.mean(xf * xf, axis=-1, keepdims=True) + 1e-05)
    normed = (xf * norm_gain).astype(jnp.bfloat16)

    def contract_all(pieces):
        return tuple(
            (jnp.dot(normed, piece, preferred_element_type=jnp.float32) for piece in pieces)
        )

    conv_sums = contract_all(
        (
            lax.all_gather(conv_b_w, "sp", axis=0, tiled=True),
            lax.all_gather(conv_c_w, "sp", axis=0, tiled=True),
            lax.all_gather(conv_x_w, "sp", axis=0, tiled=True),
        )
    )
    attn_sums = contract_all(
        (
            lax.all_gather(query_w, "sp", axis=0, tiled=True),
            lax.all_gather(key_w, "sp", axis=0, tiled=True),
            lax.all_gather(value_w, "sp", axis=0, tiled=True),
        )
    )
    sums = conv_sums + attn_sums
    gate_b, gate_c, conv_in, query, key, value = [
        (total * scale_rows).astype(jnp.bfloat16) for total in sums
    ]
    taps = conv_taps.shape[0]
    channels = conv_in.shape[1]
    conv_src = (gate_c.astype(jnp.float32) * conv_in.astype(jnp.float32)).astype(jnp.bfloat16)
    earlier = passed_along(conv_src[count - (taps - 1) :], "sp", 1)
    padded = jnp.concatenate([earlier, conv_src], axis=0)
    filtered = jnp.zeros((count, channels), jnp.float32)
    for tap in range(taps):
        filtered = filtered + conv_taps[tap][None, :] * padded[tap : tap + count].astype(
            jnp.float32
        )
    conv_out = (gate_b.astype(jnp.float32) * filtered).astype(jnp.bfloat16)
    heads_dev = gate_cache.shape[1]
    kv_dev = key.shape[1] // HD
    group = heads_dev // kv_dev
    half = count // 2
    sp_index = lax.axis_index("sp")
    own_start = sp_index * count
    scale = HD ** (-0.5)
    later_query = query[half:]
    later_start = own_start + half

    def prepare(q_rows, begin):
        heads_q = q_rows.reshape(half, kv_dev, group, HD)
        q_gate = lax.dynamic_slice_in_dim(gate_cache, begin, half, 0).T.reshape(
            kv_dev, group, half, 1
        )
        q_pos = begin + jnp.arange(half, dtype=jnp.int32)
        return (heads_q, q_gate, q_pos)

    sides = (prepare(query[:half], own_start), prepare(later_query, later_start))

    def absorb(carry, side, key_rows, value_rows, begin):
        heads_q, q_gate, q_pos = side
        run_max, run_sum, acc = carry
        width = key_rows.shape[0]
        key_heads = key_rows.reshape(width, kv_dev, HD)
        value_heads = value_rows.reshape(width, kv_dev, HD)
        score = (
            jnp.einsum("qgjd,kgd->gjqk", heads_q, key_heads, preferred_element_type=jnp.float32)
            * scale
        )
        key_gate = lax.dynamic_slice_in_dim(gate_cache, begin, width, 0).T.reshape(
            kv_dev, group, 1, width
        )
        score = score + q_gate - key_gate
        mask = (begin + jnp.arange(width, dtype=jnp.int32))[None, :] <= q_pos[:, None]
        score = jnp.where(mask, score, -1e30)
        new_max = jnp.maximum(run_max, jnp.max(score, axis=-1))
        weight = jnp.where(mask, jnp.exp(score - new_max[..., None]), 0.0)
        factor = jnp.exp(run_max - new_max)
        new_sum = run_sum * factor + jnp.sum(weight, axis=-1)
        product = jnp.einsum(
            "gjqk,kgd->gjqd",
            weight.astype(jnp.bfloat16),
            value_heads,
            preferred_element_type=jnp.float32,
        )
        return (new_max, new_sum, acc * factor[..., None] + product)

    def guarded(carry, side, key_rows, value_rows, begin):

        def visit_rows(state):
            return absorb(state, side, key_rows, value_rows, begin)

        def keep(state):
            return state

        return lax.cond(begin <= side[2][half - 1], visit_rows, keep, carry)

    def absorb_both(carry, key_rows, value_rows, begin):
        return (
            guarded(carry[0], sides[0], key_rows, value_rows, begin),
            guarded(carry[1], sides[1], key_rows, value_rows, begin),
        )

    def fresh():
        return (
            jnp.full((kv_dev, group, half), -1e30, jnp.float32),
            jnp.zeros((kv_dev, group, half), jnp.float32),
            jnp.zeros((kv_dev, group, half, HD), jnp.float32),
        )

    key_rows = lax.all_gather(key, "sp", axis=0, tiled=True)
    value_rows = lax.all_gather(value, "sp", axis=0, tiled=True)
    width = key_rows.shape[0]
    step = 512
    key_blocks = key_rows.reshape(width // step, step, key_rows.shape[1])
    value_blocks = value_rows.reshape(width // step, step, value_rows.shape[1])
    firsts = step * jnp.arange(width // step, dtype=jnp.int32)

    def visit(state, inputs):
        return (absorb_both(state, inputs[0], inputs[1], inputs[2]), None)

    result, _ = lax.scan(visit, (fresh(), fresh()), (key_blocks, value_blocks, firsts))

    def finish(state):
        run_max, run_sum, acc = state
        out = (
            (acc / run_sum[..., None])
            .transpose(2, 0, 1, 3)
            .reshape(half, heads_dev * HD)
            .astype(jnp.bfloat16)
        )
        lse = (run_max + jnp.log(run_sum)).transpose(2, 0, 1).reshape(half, heads_dev)
        return (out, lse)

    early_out, early_lse = finish(result[0])
    later_out, later_lse = finish(result[1])
    attn_out = jnp.concatenate([early_out, later_out], axis=0)
    log_total = jnp.concatenate([early_lse, later_lse], axis=0)
    term = jnp.dot(conv_out, out_conv_w, preferred_element_type=jnp.float32)
    mixed = lax.psum_scatter(
        (term + jnp.dot(attn_out, out_attn_w, preferred_element_type=jnp.float32)).astype(
            jnp.bfloat16
        ),
        "tp",
        scatter_dimension=0,
        tiled=True,
    )
    return (mixed, log_total)


def shape(dims, dtype=jnp.bfloat16):
    return jax.ShapeDtypeStruct(dims, dtype)


def run(kernel, operands, outs, scratch, flops, nbytes, mib, spec=VMEM):
    def placed(*refs):
        kernel(tuple(lax.axis_index(axis) for axis in ("sp", "tp", "grp")), *refs)

    return pl.pallas_call(
        placed,
        out_shape=outs,
        in_specs=[spec] * len(operands),
        out_specs=jax.tree.map(lambda unused: VMEM, outs),
        scratch_shapes=scratch,
        cost_estimate=pl.CostEstimate(flops=flops, bytes_accessed=nbytes, transcendentals=0),
        compiler_params=pltpu.CompilerParams(vmem_limit_bytes=mib << 20),
    )(*operands)


def low_half(width):
    return lax.broadcasted_iota(jnp.int32, (1, width), 1) < width // 2


def pack_kernel(n, at, *rest):
    sources, rest = rest[:6], rest[6:]
    outs, held, sems = rest[:n], rest[n : n + 6], rest[n + 6]
    own, part = at[0], at[2]
    copies = [
        pltpu.make_async_copy(source, ref, sems.at[index])
        for index, (source, ref) in enumerate(zip(sources, held))
    ]
    for copy in copies:
        copy.start()
    for copy in copies:
        copy.wait()
    b_ref, c_ref, x_ref, q_ref, k_ref, v_ref = held

    def both(ref):
        turned = ref[...].astype(jnp.float32)
        return jnp.concatenate([turned, turned], axis=0).T

    key, value = both(k_ref), both(v_ref)
    low = low_half(LANES)
    for step in range(n):
        to = own ^ step
        tile = pl.ds(pl.multiple_of((to // 2) * LANES, LANES), LANES)
        odd = (to % 2) == 1

        def sides(ref):
            plain = ref[:, tile].astype(jnp.float32)
            return plain, pltpu.roll(plain, LANES // 2, 1)

        def lower(ref):
            plain, rolled = sides(ref)
            return jnp.where(odd, rolled, plain)

        def upper(ref):
            plain, rolled = sides(ref)
            return jnp.where(odd, plain, rolled)

        tiles = (
            jnp.where(low, lower(b_ref), upper(q_ref)),
            jnp.where(low, lower(c_ref), key),
            jnp.where(low, lower(x_ref), value),
        )
        for index, full in enumerate(tiles):
            columns = slice(index * LANES, (index + 1) * LANES)
            full = full.astype(jnp.bfloat16)
            out = outs[step]
            if step == 0:
                out[:, columns] = full
            else:
                half = out.shape[0]
                out[:, columns] = jnp.where(part == 0, full[:half], full[half:])


def order_kernel(n, at, conv_w, attn_w, out):
    own = at[0]
    for step in range(n):
        begin = pl.multiple_of((own ^ step) * HD, HD)
        out[step * LANES : step * LANES + HD, :] = conv_w[pl.ds(begin, HD), :]
        out[step * LANES + HD : (step + 1) * LANES, :] = attn_w[pl.ds(begin, HD), :]


def columns_of(ref, start, depth):
    return ref[:, pl.ds(pl.multiple_of(start, depth), depth)]


def norm_kernel(kinds, places, m, at, gain_ref, weight, *rest):
    parts, rest = rest[: len(places)], rest[len(places) :]
    pieces, (normed, scales, total) = rest[: len(kinds)], rest[len(kinds) :]
    own, column = at[0], at[1]
    gain = gain_ref[...]
    for (index, begin), ref in zip(places, parts):
        count = ref.shape[0]
        rows = pl.ds(pl.multiple_of((column ^ index) * m + begin, count), count)
        xf = ref[...].astype(jnp.float32)
        scale = lax.rsqrt(jnp.mean(xf * xf, axis=-1, keepdims=True) + EPS)
        scales[rows, :] = jnp.broadcast_to(scale, (count, LANES))
        normed[rows, :] = (xf * gain).astype(jnp.bfloat16)
    depth = weight.shape[0]
    first = jnp.dot(
        columns_of(normed, own * depth, depth), weight[...], preferred_element_type=jnp.float32
    )
    if kinds:
        first = first + terms(at, normed, [(*kind, ref) for kind, ref in zip(kinds, pieces)])
    total[...] = first


def terms(at, normed, pieces):
    own, part = at[0], at[2]
    total = None
    for step, handed, ref in pieces:
        half = ref.shape[0]
        start = (own ^ step) * (2 * half) + ((1 - part) if handed else part) * half
        term = jnp.dot(
            columns_of(normed, start, half), ref[...], preferred_element_type=jnp.float32
        )
        total = term if total is None else total + term
    return total


def join_kernel(blocks, kinds, at, *rest):
    normed, totals = rest[:blocks], rest[blocks : 2 * blocks]
    pieces, outs = rest[2 * blocks : -blocks], rest[-blocks:]
    listed = [(*kind, ref) for kind, ref in zip(kinds, pieces)]
    for index in range(blocks):
        outs[index][...] = totals[index][...] + terms(at, normed[index], listed)


def mix_kernel(n, kinds, at, *rest):
    normed, totals, scales = rest[:n], rest[n : 2 * n], rest[2 * n : 3 * n]
    pieces, rest = rest[3 * n : 3 * n + len(kinds)], rest[3 * n + len(kinds) :]
    taps_ref, gate_ref = rest[:2]
    outs, (held, source, mixed, lse) = rest[2 : 2 + n], rest[2 + n :]
    own = at[0]
    count = normed[0].shape[0]
    rows_all = n * count
    listed = [(*kind, ref) for kind, ref in zip(kinds, pieces)]
    for step in range(n):
        begin = pl.multiple_of((own ^ step) * count, count)
        total = totals[step][...] + terms(at, normed[step], listed)
        held[pl.ds(begin, count), :] = (total * scales[step][:, :1]).astype(jnp.bfloat16)
    low = low_half(LANES)
    lead = source.shape[0] - rows_all
    source[:lead, :] = jnp.zeros((lead, LANES), jnp.float32)
    gated = held[:, LANES : 2 * LANES].astype(jnp.float32) * held[:, 2 * LANES :].astype(
        jnp.float32
    )
    source[lead:, :] = gated.astype(jnp.bfloat16).astype(jnp.float32)
    taps_n = taps_ref.shape[0]
    tile = pl.ds(pl.multiple_of((own // 2) * LANES, LANES), LANES)
    taps = taps_ref[:, tile]
    taps = jnp.where((own % 2) == 1, pltpu.roll(taps, LANES // 2, 1), taps)
    gate_row = gate_ref[pl.ds(own, 1), :]
    scale = HD ** (-0.5)
    ahead = lax.broadcasted_iota(jnp.int32, (count, count), 0) >= lax.broadcasted_iota(
        jnp.int32, (count, count), 1
    )
    for block in range(n):
        first = block * count
        last = first + count
        filtered = jnp.zeros((count, LANES), jnp.float32)
        for tap in range(taps_n):
            begin = lead + first + tap - (taps_n - 1)
            filtered = filtered + taps[tap : tap + 1, :] * source[begin : begin + count, :]
        front = held[first:last, :LANES]
        conv = front.astype(jnp.float32) * filtered
        query = jnp.where(low, 0.0, front.astype(jnp.float32) * scale).astype(jnp.bfloat16)
        score = lax.dot_general(
            query,
            held[:last, LANES : 2 * LANES],
            (((1,), (1,)), ((), ())),
            preferred_element_type=jnp.float32,
        )
        score = score - gate_row[:, :last]
        edge = jnp.where(ahead, score[:, first:], -1e30)
        if block:
            before = score[:, :first]
            top = jnp.maximum(
                jnp.max(before, axis=-1, keepdims=True), jnp.max(edge, axis=-1, keepdims=True)
            )
            weight = jnp.concatenate([jnp.exp(before - top), jnp.exp(edge - top)], axis=1)
        else:
            top = jnp.max(edge, axis=-1, keepdims=True)
            weight = jnp.exp(edge - top)
        total = jnp.sum(weight, axis=-1, keepdims=True)
        product = jnp.dot(
            weight.astype(jnp.bfloat16),
            held[:last, 2 * LANES :],
            preferred_element_type=jnp.float32,
        )
        mixed[first:last, :] = jnp.where(low, conv, product / total).astype(jnp.bfloat16)
        lse[block : block + 1, :] = (
            jnp.broadcast_to(top + jnp.log(total), (count, LANES)).T[:1, :]
            + gate_row[:, first:last]
        )
    for step in range(n):
        to = own ^ step
        outs[step][:count, :] = mixed[pl.ds(pl.multiple_of(to * count, count), count), :]
        left, lines = lse[pl.ds(to, 1), :], []
        for _ in range(PIECES):
            piece = left.astype(jnp.bfloat16).astype(jnp.float32)
            lines += [piece[:, at : at + LANES] for at in range(0, count, LANES)]
            left = left - piece
        lines.append(jnp.zeros((outs[step].shape[0] - count - len(lines), LANES), jnp.float32))
        outs[step][count:, :] = jnp.concatenate(lines, axis=0).astype(jnp.bfloat16)


def out_kernel(n, first, at, *rest):
    parts, weights = rest[: 2 * n], rest[2 * n : 2 * n + 2]
    far, near, *logs, joined = rest[2 * n + 2 :]
    own, column = at[0], at[1]
    count, width = far.shape
    if logs:
        log_rows(n, own, parts, logs[0])
    for place, row in enumerate((column ^ 2, column)):
        begin = pl.multiple_of(row * count, count)
        for index, ref in enumerate(parts):
            joined[
                place * count : (place + 1) * count, index * LANES : (index + 1) * LANES
            ] = ref[pl.ds(begin, count), :]
    tile = 2 * LANES
    for begin in range(0, width, tile):
        columns = slice(begin, begin + tile)
        total = None
        for index, ref in enumerate(weights):
            term = jnp.dot(
                joined[:, index * n * LANES : (index + 1) * n * LANES],
                ref[:, first + begin : first + begin + tile],
                preferred_element_type=jnp.float32,
            )
            total = term if total is None else total + term
        far[:, columns] = total[:count].astype(jnp.bfloat16)
        near[:, columns] = total[count:]


def log_rows(n, own, parts, logs):
    positions = logs.shape[1]
    lines = positions // LANES
    for step in range(n):
        tail = parts[step][positions:, :].astype(jnp.float32)
        row = []
        for line in range(lines):
            value = tail[line : line + 1]
            for piece in range(1, PIECES):
                place = piece * lines + line
                value = value + tail[place : place + 1]
            row.append(value)
        logs[pl.ds(own ^ step, 1), :] = jnp.concatenate(row, axis=1)


def sum_kernel(near0, near1, far0, far1, out):
    width = far0.shape[1]
    for index, (near, far) in enumerate(((near0, far0), (near1, far1))):
        total = near[...] + far[...].astype(jnp.float32)
        out[:, index * width : (index + 1) * width] = total.astype(jnp.bfloat16)


def split_kernel(at, whole, early, late):
    count = early.shape[0]
    early[...] = whole[:count]
    late[...] = whole[count:]


def pick_part_kernel(n, begin, at, inner, outer, out):
    own = at[0]
    end = (own == 0) | (own == n - 1)

    @pl.when(end)
    def take_outer():
        out[...] = outer[...]

    @pl.when(jnp.logical_not(end))
    def take_inner():
        out[...] = inner[begin : begin + out.shape[0]]


def pick_kernel(n, at, inner, outer, out):
    own = at[0]
    end = (own == 0) | (own == n - 1)

    @pl.when(end)
    def take_outer():
        out[...] = outer[...]

    @pl.when(jnp.logical_not(end))
    def take_inner():
        out[...] = inner[...]


def by_columns(
    tokens,
    norm_gain,
    conv_b_w,
    conv_c_w,
    conv_x_w,
    query_w,
    key_w,
    value_w,
    conv_taps,
    gate_cache,
    out_conv_w,
    out_attn_w,
):
    n, n_tp = lax.axis_size("sp"), lax.axis_size("tp")
    swap = lambda bit: [(i, i ^ bit) for i in range(n)]
    last = n - 1
    outward = [(n // 2, last), (n // 2 - 1, 0)]
    inward = [(0, n // 2), (last, n // 2 - 1)]
    middle = [(n // 2 - 1, n // 2), (n // 2, n // 2 - 1)]
    m, d = tokens.shape
    depth, width = conv_b_w.shape
    packed = 3 * LANES
    half = depth // 2
    count = m * n_tp
    rows = n * count
    gain = norm_gain.reshape(1, d)
    z1 = lax.ppermute(tokens, "sp", swap(1))
    z3a = lax.ppermute(tokens, "sp", middle)
    z2a = lax.ppermute(tokens, "sp", inward)
    own_w, *sends = run(
        functools.partial(pack_kernel, n),
        (conv_b_w, conv_c_w, conv_x_w, query_w, key_w.T, value_w.T),
        [shape((depth, packed))] + [shape((half, packed))] * (n - 1),
        [pltpu.VMEM((depth, width), jnp.bfloat16)] * 4
        + [pltpu.VMEM((key_w.shape[1], depth), jnp.bfloat16)] * 2
        + [pltpu.SemaphoreType.DMA((6,))],
        depth * packed * n,
        6 * depth * width,
        PACK_MIB,
        pl.BlockSpec(memory_space=pltpu.HBM),
    )
    came = {k: lax.ppermute(sends[k - 1], "sp", swap(k)) for k in range(1, n)}
    given = {k: lax.ppermute(came[k], "grp", [(0, 1), (1, 0)]) for k in range(1, n)}
    z2b = lax.ppermute(z3a, "sp", outward)
    part = m // 2
    z2a_parts = run(split_kernel, (z2a,), [shape((part, d))] * 2, [], 0, 4 * m * d, 2)
    z3b = [lax.ppermute(z2a_parts[i], "sp", outward) for i in range(2)]

    def pick(inner, outer):
        return run(
            functools.partial(pick_kernel, n), (inner, outer), shape((m, d)), [], 0, 6 * m * d, 2
        )

    z2 = pick(z2a, z2b)
    z3 = []
    for i in range(2):
        z3.append(
            run(
                functools.partial(pick_part_kernel, n, i * part),
                (z3a, z3b[i]),
                shape((part, d)),
                [],
                0,
                4 * m * d,
                2,
            )
        )
    out_w = run(
        functools.partial(order_kernel, n),
        (out_conv_w, out_attn_w),
        shape((n * LANES, d)),
        [],
        0,
        4 * n * LANES * d,
        4,
    )
    out_w_other = lax.ppermute(out_w, "tp", swap(1))
    piece = lambda kind: (given if kind[1] else came)[kind[0]]
    normed, scales, totals = [], [], []
    for k, mine in enumerate(([tokens], [z1], [z2], z3)):
        kinds = EARLY if k == n - 1 else ()
        places, arrays = [], []
        for i, value in enumerate(mine):
            over = lax.ppermute(value, "tp", swap(2))
            side = lax.ppermute(value, "tp", swap(1))
            cross = lax.ppermute(over, "tp", swap(1))
            begin = i * value.shape[0]
            places += [(0, begin), (1, begin), (2, begin), (3, begin)]
            arrays += [value, side, over, cross]
        results = run(
            functools.partial(norm_kernel, kinds, places, m),
            (gain, own_w, *arrays, *(piece(kind) for kind in kinds)),
            [
                shape((count, d)),
                shape((count, LANES), jnp.float32),
                shape((count, packed), jnp.float32),
            ],
            [],
            2 * count * (depth + half * len(kinds)) * packed,
            4 * count * d,
            4,
        )
        normed.append(results[0])
        scales.append(results[1])
        totals.append(results[2])
    blocks = n - 1
    joined = run(
        functools.partial(join_kernel, blocks, EARLY),
        (*normed[:blocks], *totals[:blocks], *(piece(kind) for kind in EARLY)),
        [shape((count, packed), jnp.float32)] * blocks,
        [],
        2 * blocks * count * half * len(EARLY) * packed,
        8 * rows * packed,
        4,
    )
    totals = [*joined, totals[-1]]
    late = LATE
    extra = -(-PIECES * count // (SUBLANES * LANES)) * SUBLANES
    results = run(
        functools.partial(mix_kernel, n, late),
        (
            *normed,
            *totals,
            *scales,
            *(piece(kind) for kind in late),
            conv_taps,
            gate_cache.T,
        ),
        [shape((count + extra, LANES))] * n,
        [
            pltpu.VMEM((rows, packed), jnp.bfloat16),
            pltpu.VMEM((rows + 8, LANES), jnp.float32),
            pltpu.VMEM((rows, LANES), jnp.bfloat16),
            pltpu.VMEM((n, count), jnp.float32),
        ],
        4 * rows * rows * LANES,
        2 * rows * packed,
        12,
    )
    parts = [results[0]] + [lax.ppermute(results[k], "sp", swap(k)) for k in range(1, n)]

    other = [lax.ppermute(part, "tp", swap(1)) for part in parts]
    near, far = [], []
    wide = d // 2
    for i in range(2):
        logs = [shape((n, count), jnp.float32)] * i
        results = run(
            functools.partial(out_kernel, n, i * wide),
            (*parts, *other, out_w, out_w_other),
            [shape((m, wide)), shape((m, wide), jnp.float32), *logs],
            [pltpu.VMEM((2 * m, 2 * n * LANES), jnp.bfloat16)],
            4 * m * n * LANES * d,
            2 * n * LANES * d,
            8,
        )
        far.append(lax.ppermute(results[0], "tp", swap(2)))
        near.append(results[1])
    log_total = results[2].T
    mixed = pl.pallas_call(
        sum_kernel,
        out_shape=shape((m, d)),
        in_specs=[VMEM] * 4,
        out_specs=VMEM,
        name="total",
        cost_estimate=pl.CostEstimate(flops=4 * m * d, bytes_accessed=10 * m * d, transcendentals=0),
        compiler_params=pltpu.CompilerParams(vmem_limit_bytes=4 << 20),
    )(*near, *far)
    return (mixed, log_total)


PIECES = 3
PACK_MIB = 58
SUBLANES = 16
EARLY = ((1, False), (3, False), (2, False), (1, True), (3, True))
LATE = ((2, True),)


def on_device(*operands):
    tokens, key_w, gate_cache = operands[0], operands[6], operands[9]
    n, n_tp, n_grp = (lax.axis_size(name) for name in ("sp", "tp", "grp"))
    channels = operands[2].shape[1]
    heads = gate_cache.shape[1]
    fits = (
        n == heads == 4
        and n_tp == 4
        and n_grp == 2
        and key_w.shape[1] == HD
        and channels == n * HD
        and 2 * HD == LANES
        and gate_cache.shape[0] == n * n_tp * tokens.shape[0]
    )
    return (by_columns if fits else by_rows)(*operands)


def solution(mesh):
    placed = (
        P(("grp", "sp", "tp"), None),
        P(),
        P("sp", "tp"),
        P("sp", "tp"),
        P("sp", "tp"),
        P("sp", "tp"),
        P("sp", "tp"),
        P("sp", "tp"),
        P(None, "tp"),
        P("grp", "tp"),
        P("tp", None),
        P("tp", None),
    )
    return jax.shard_map(
        on_device,
        mesh=mesh,
        in_specs=placed,
        out_specs=(P(("grp", "sp", "tp"), None), P(("grp", "sp"), "tp")),
        check_vma=False,
    )
```
